32 devices in a mesh: grp: 2 (over y), ep: 8 (over z, x), tp: 2 (over core).
Axes of the slice: x: 2, y: 2, z: 4, core: 2. Of those that a mesh axis runs over, the one named last changes fastest.
Arguments:
- tokens: bfloat16 [512, 1024], P(('grp', 'ep', 'tp')), parts along dimension 0, may hold values from -1.75 to 1.75
- latent_cache: bfloat16 [512, 1024, 256], P(('grp', 'ep', 'tp')), parts along dimension 0, may hold values from -6 to 6
- rope_cache: bfloat16 [512, 1024, 32], P(('grp', 'ep', 'tp')), parts along dimension 0, may hold values from -1200 to 1200
- lengths: int32 [512], P(('grp', 'ep', 'tp')), parts along dimension 0, may hold values from 128 to 1024
- expert_ids: int32 [512, 4], P(('grp', 'ep', 'tp')), parts along dimension 0, may hold values from 0 to 15, all different within a row; in each aligned block of 16 rows (0 to 15, 16 to 31, ...) at most 4 rows name the same one
- route_weights: float32 [512, 4], P(('grp', 'ep', 'tp')), parts along dimension 0, may hold values from 0.1 to 1
- g_attn: float32 [1024], replicated, may hold values from 0.1 to 1.9
- w_query_down: bfloat16 [1024, 256], replicated, may hold values from -0.1875 to 0.1875
- g_query: float32 [256], replicated, may hold values from 0.1 to 1.9
- w_latent_down: bfloat16 [1024, 256], replicated, may hold values from -0.1875 to 0.1875
- g_latent: float32 [256], replicated, may hold values from 0.1 to 1.9
- w_rope_key: bfloat16 [1024, 32], replicated, may hold values from -0.1875 to 0.1875
- w_query: bfloat16 [256, 1024], replicated, may hold values from -0.375 to 0.375
- w_query_rope: bfloat16 [256, 512], replicated, may hold values from -0.375 to 0.375
- w_key_up: bfloat16 [256, 1024], replicated, may hold values from -0.875 to 0.875
- w_value_up: bfloat16 [256, 1024], replicated, may hold values from -0.375 to 0.375
- w_out: bfloat16 [1024, 1024], replicated, may hold values from -0.1875 to 0.1875
- g_ffn: float32 [1024], replicated, may hold values from 0.1 to 1.9
- w_expert_gate: bfloat16 [16, 1024, 256], P('ep', None, 'tp'), may hold values from -0.1875 to 0.1875
- w_expert_up: bfloat16 [16, 1024, 256], P('ep', None, 'tp'), may hold values from -0.1875 to 0.1875
- w_expert_down: bfloat16 [16, 256, 1024], P('ep', 'tp'), may hold values from -0.375 to 0.375
- w_shared_gate: bfloat16 [1024, 256], replicated, may hold values from -0.1875 to 0.1875
- w_shared_up: bfloat16 [1024, 256], replicated, may hold values from -0.1875 to 0.1875
- w_shared_down: bfloat16 [256, 1024], replicated, may hold values from -0.375 to 0.375
Outputs:
- mixed_out: bfloat16 [512, 1024], P(('grp', 'ep', 'tp')), parts along dimension 0
- new_entry: bfloat16 [512, 288], P(('grp', 'ep', 'tp')), parts along dimension 0
The draws below stay inside these ranges and needn't reach their ends.
There are 2 independent parts, one for each index of `grp`. The reference program is written for one: setup_inputs(seed, part) draws one part's arguments, and reference() takes and returns one part's arrays. A program takes and returns all parts, laid end to end along the dimension named above; an argument that names none is the same for every part. Nothing has to cross between parts.
Inputs may be any that keep to these rules, and one draw needn't show every extreme that they name: `expert_ids`: each row names 4 different experts. In the aligned blocks of rows that one device holds (one block for each device of ep and tp together), no expert is named by more than 4 rows, a bound that some block reaches.
All inputs are finite; a program needn't handle non-finite values.
Results may differ from the reference program's by a relative error of at most 0.03.
Values may be sent and summed in bfloat16 or wider, within the bound.
A program may use at most 64 MiB of HBM per device.

```python
import math
import jax
import jax.numpy as jnp
import numpy as np
from jax import lax

D = 1024
HEADS = 16
QLORA = 256
KVLORA = 256
NOPE = 64
ROPE = 32
VDIM = 64
EFF = 256
SFF = 256
TOPK = 4
SEQS = 32
CACHE_LEN = 1024
EXPERTS = 16
CAP = 4
BATCH = 256
N_EP = 8
N_TP = 2


def draw_rope_cache(key, part):
    base_draw = jax.random.truncated_normal(key, -4.0, 4.0, (BATCH, CACHE_LEN, ROPE), jnp.float32)
    return base_draw.astype(jnp.bfloat16)


def plant(result, stream_key, least, largest):
    longest = result.shape.index(max(result.shape))
    spots = []
    for shift in (0, 1):
        where = [jax.random.randint(jax.random.fold_in(stream_key, axis), (), 0, length) for axis, length in enumerate(result.shape)]
        where[longest] = (where[longest] + shift) % result.shape[longest]
        spots.append(tuple(where))
    return result.at[spots[0]].set(least).at[spots[1]].set(largest)


def level_of(stream_key, shape, pieces, low, high):
    factor_of = 1.0
    for position, blocks in pieces:
        draws = jax.random.uniform(jax.random.fold_in(jax.random.fold_in(stream_key, 6), position), (blocks,), jnp.float32, low / len(pieces), high / len(pieces))
        factor_of = factor_of * jnp.repeat(jnp.exp(draws), shape[position] // blocks).reshape((-1,) + (1,) * (len(shape) - 1 - position))
    return factor_of


def routed_block(rng, own, number, rows, count, top, limit, slope):
    ranking = jax.random.permutation(rng, count)
    crowded, common = portions_of(count, rows * top, limit, slope, True), portions_of(count, rows * top, limit, slope, False)
    places = jnp.arange(count)

    def named(sizes, rotation):
        used = int((sizes > 0).sum())
        fixed = max(1, used // 4)
        shifted = fixed + (places - fixed + rotation * (used - fixed)) % max(1, count - fixed)
        return jnp.zeros((count,), jnp.int32).at[ranking[jnp.where(places < fixed, places, shifted)]].set(jnp.asarray(sizes, jnp.int32))

    sizes = jnp.where(number % 4 == 0, named(crowded, number // 4), named(common, number - number // 4 - 1))
    mixed = jax.random.permutation(jax.random.fold_in(own, 3), count)
    donor, taker = mixed[0:count // 2 * 2:2], mixed[1:count // 2 * 2:2]
    room = jnp.minimum(sizes[donor] - 1, limit - sizes[taker]) // 2
    room = jnp.where((donor == ranking[0]) | (taker == ranking[0]) | (sizes[taker] == 0), 0, jnp.maximum(room, 0))
    shifted = jax.random.randint(jax.random.fold_in(own, 4), (count // 2,), 0, 1 << 20) % (room + 1)
    sizes = sizes.at[donor].add(-shifted).at[taker].add(shifted)
    members = jnp.searchsorted(jnp.cumsum(sizes), jnp.arange(rows * top), side="right").astype(jnp.int32)
    listing = members.reshape(top, rows).T
    listing = listing[jax.random.permutation(jax.random.fold_in(own, 1), rows)]
    rotation = jax.random.randint(jax.random.fold_in(own, 2), (rows, 1), 0, top)
    return jnp.take_along_axis(listing, (jnp.arange(top)[None, :] + rotation) % top, axis=1)


def portions_of(number_of, total, reach, lean, full):
    portions = [(1 << 20) // math.isqrt(standing ** lean) + 1 for standing in range(1, number_of + 1)]
    largest = reach if full else min(reach, max(-(-total // number_of), total * portions[0] // sum(portions)))
    least = 1 if total - largest >= number_of - 1 else 0
    counts, surplus = [largest] + [least] * (number_of - 1), total - largest - least * (number_of - 1)
    while surplus > 0:
        free = [i for i in range(1, number_of) if counts[i] < largest] or [i for i in range(1, number_of) if counts[i] < reach]
        pool, budget = sum([portions[i] for i in free]), surplus
        for i in free:
            more = min(reach - counts[i], max(1, budget * portions[i] // pool), surplus)
            counts[i] = counts[i] + more
            surplus = surplus - more
    return np.array(counts)


def noise(stream_key, shape, scale, reach, pieces=(), kind=jnp.bfloat16):
    values = jax.random.normal(stream_key, shape, jnp.float32) * scale
    if len(pieces) > 0:
        values = level_of(stream_key, shape, pieces, -0.22, 0.18) * values
    return jnp.clip(values, min=-reach, max=reach).astype(kind)


def setup_inputs(seed: int = 0, part: int = 0) -> dict:
    seeds = jax.random.split(jax.random.key(seed), 25)
    part_keys = jax.random.split(jax.random.fold_in(seeds[24], part), 25)
    tokens = noise(part_keys[0], (BATCH, D), 0.3, 1.75, ((0, 16),))
    latent_cache = noise(part_keys[1], (BATCH, CACHE_LEN, KVLORA), 1.0, 6.0, ((0, 16),))
    rope_cache = draw_rope_cache(jax.random.fold_in(jax.random.fold_in(seeds[24], part), 71), part)
    lengths = plant(jax.random.randint(part_keys[3], (BATCH,), CACHE_LEN // 8, CACHE_LEN + 1), jax.random.fold_in(part_keys[3], 1), CACHE_LEN // 8, CACHE_LEN).astype(jnp.int32)
    expert_ids_keys = jax.random.split(jax.random.fold_in(part_keys[4], 1), BATCH // (SEQS // N_TP))
    expert_ids_turns = jax.random.permutation(jax.random.fold_in(part_keys[4], 3), BATCH // (SEQS // N_TP))
    expert_ids = jax.vmap(lambda own, number: routed_block(jax.random.fold_in(part_keys[4], 2), own, number, SEQS // N_TP, EXPERTS, TOPK, CAP, 2))(expert_ids_keys, expert_ids_turns).reshape((BATCH, TOPK))
    route_weights = jnp.clip(jnp.exp(math.log(1.0) - 2.3025851 * jax.random.uniform(part_keys[5], (BATCH, TOPK), jnp.float32) ** level_of(part_keys[5], (BATCH, TOPK), ((0, 16),), -0.2, 0.2)), 0.1, 1.0)
    g_attn = jnp.clip(1.0 + 0.18 * jax.random.normal(seeds[6], (D,), jnp.float32), 0.1, 1.9)
    w_query_down = noise(seeds[7], (D, QLORA), D ** -0.5, 0.1875)
    g_query = jnp.clip(1.0 + 0.18 * jax.random.normal(seeds[8], (QLORA,), jnp.float32), 0.1, 1.9)
    w_latent_down = noise(seeds[9], (D, KVLORA), D ** -0.5, 0.1875)
    g_latent = jnp.clip(1.0 + 0.18 * jax.random.normal(seeds[10], (KVLORA,), jnp.float32), 0.1, 1.9)
    w_rope_key = noise(seeds[11], (D, ROPE), D ** -0.5, 0.1875)
    w_query = noise(seeds[12], (QLORA, HEADS * NOPE), QLORA ** -0.5, 0.375)
    w_query_rope = noise(seeds[13], (QLORA, HEADS * ROPE), QLORA ** -0.5, 0.375)
    w_key_up = noise(seeds[14], (KVLORA, HEADS * NOPE), 0.15, 0.875)
    w_value_up = noise(seeds[15], (KVLORA, HEADS * VDIM), KVLORA ** -0.5, 0.375)
    w_out = noise(seeds[16], (HEADS * VDIM, D), (HEADS * VDIM) ** -0.5, 0.1875)
    g_ffn = jnp.clip(1.0 + 0.18 * jax.random.normal(seeds[17], (D,), jnp.float32), 0.1, 1.9)
    w_expert_gate = noise(seeds[18], (EXPERTS, D, EFF), D ** -0.5, 0.1875, ((0, 8), (2, 2)))
    w_expert_up = noise(seeds[19], (EXPERTS, D, EFF), D ** -0.5, 0.1875, ((0, 8), (2, 2)))
    w_expert_down = noise(seeds[20], (EXPERTS, EFF, D), EFF ** -0.5, 0.375, ((0, 8), (1, 2)))
    w_shared_gate = noise(seeds[21], (D, SFF), D ** -0.5, 0.1875)
    w_shared_up = noise(seeds[22], (D, SFF), D ** -0.5, 0.1875)
    w_shared_down = noise(seeds[23], (SFF, D), SFF ** -0.5, 0.375)
    return {"tokens": tokens, "latent_cache": latent_cache, "rope_cache": rope_cache, "lengths": lengths, "expert_ids": expert_ids, "route_weights": route_weights, "g_attn": g_attn, "w_query_down": w_query_down, "g_query": g_query, "w_latent_down": w_latent_down, "g_latent": g_latent, "w_rope_key": w_rope_key, "w_query": w_query, "w_query_rope": w_query_rope, "w_key_up": w_key_up, "w_value_up": w_value_up, "w_out": w_out, "g_ffn": g_ffn, "w_expert_gate": w_expert_gate, "w_expert_up": w_expert_up, "w_expert_down": w_expert_down, "w_shared_gate": w_shared_gate, "w_shared_up": w_shared_up, "w_shared_down": w_shared_down}


norm_eps = 1e-06
rope_theta = 10000.0
masked_score = -1e+30

def rms_scale(values, gain_vec):
    mean_square = lax.optimization_barrier(jnp.mean(values * values, axis=-1, keepdims=True))
    return values * lax.rsqrt(mean_square + norm_eps) * gain_vec.astype(jnp.float32)

def rotate(values, positions):
    half_width = values.shape[-1] // 2
    frequency = rope_theta ** (-jnp.arange(half_width, dtype=jnp.float32) / half_width)
    angles = positions.astype(jnp.float32)[:, None] * frequency[None, :]
    angles = angles.reshape(angles.shape[:1] + (1,) * (values.ndim - 2) + (half_width,))
    cosine = jnp.cos(angles)
    sine_part = jnp.sin(angles)
    first_half = values[..., :half_width]
    second_half = values[..., half_width:]
    return jnp.concatenate([first_half * cosine - second_half * sine_part, first_half * sine_part + second_half * cosine], axis=-1)

def attend_block(block_args):
    query_latent, query_rope, cache_latent, cache_rope, length = block_args
    scores = (jnp.einsum('shc,stc->sht', query_latent.astype(jnp.float32), cache_latent.astype(jnp.float32)) + jnp.einsum('shr,str->sht', query_rope.astype(jnp.float32), cache_rope.astype(jnp.float32))) * (NOPE + ROPE) ** (-0.5)
    live_mask = jnp.arange(CACHE_LEN, dtype=jnp.int32)[None, None, :] < length[:, None, None]
    row_max = lax.optimization_barrier(jnp.max(jnp.where(live_mask, scores, masked_score), axis=2, keepdims=True))
    weights = jnp.where(live_mask, jnp.exp(scores - row_max), 0.0)
    weight_sum = lax.optimization_barrier(jnp.sum(weights, axis=2))
    rounded = lax.optimization_barrier(weights.astype(jnp.bfloat16)).astype(jnp.float32)
    mixed_latent = jnp.einsum('sht,stc->shc', rounded, cache_latent.astype(jnp.float32))
    return (mixed_latent / weight_sum[:, :, None]).astype(jnp.bfloat16)

def reference(tokens, latent_cache, rope_cache, lengths, expert_ids, route_weights, g_attn, w_query_down, g_query, w_latent_down, g_latent, w_rope_key, w_query, w_query_rope, w_key_up, w_value_up, w_out, g_ffn, w_expert_gate, w_expert_up, w_expert_down, w_shared_gate, w_shared_up, w_shared_down):
    row_count = tokens.shape[0]
    normed = rms_scale(tokens.astype(jnp.float32), g_attn).astype(jnp.bfloat16)
    query_low = rms_scale(jnp.dot(normed, w_query_down, preferred_element_type=jnp.float32), g_query).astype(jnp.bfloat16)
    latent_new = rms_scale(jnp.dot(normed, w_latent_down, preferred_element_type=jnp.float32), g_latent).astype(jnp.bfloat16)
    key_new = rotate(jnp.dot(normed, w_rope_key, preferred_element_type=jnp.float32), lengths).astype(jnp.bfloat16)
    new_entry = jnp.concatenate([latent_new, key_new], axis=1)
    query_nope = jnp.dot(query_low, w_query, preferred_element_type=jnp.float32).astype(jnp.bfloat16)
    query_nope = query_nope.reshape(row_count, HEADS, NOPE)
    query_turn = jnp.dot(query_low, w_query_rope, preferred_element_type=jnp.float32).reshape(row_count, HEADS, ROPE)
    query_rope = rotate(query_turn, lengths).astype(jnp.bfloat16)
    query_latent = jnp.einsum('bhn,chn->bhc', query_nope.astype(jnp.float32), w_key_up.reshape(KVLORA, HEADS, NOPE).astype(jnp.float32)).astype(jnp.bfloat16)
    block_size = SEQS // N_TP
    block_count = row_count // block_size
    latent_mix = lax.map(attend_block, (query_latent.reshape(block_count, block_size, HEADS, KVLORA), query_rope.reshape(block_count, block_size, HEADS, ROPE), latent_cache.reshape(block_count, block_size, CACHE_LEN, KVLORA), rope_cache.reshape(block_count, block_size, CACHE_LEN, ROPE), lengths.reshape(block_count, block_size))).reshape(row_count, HEADS, KVLORA)
    value_heads = jnp.einsum('bhc,chv->bhv', latent_mix.astype(jnp.float32), w_value_up.reshape(KVLORA, HEADS, VDIM).astype(jnp.float32)).astype(jnp.bfloat16)
    attn_out = jnp.dot(value_heads.reshape(row_count, HEADS * VDIM), w_out, preferred_element_type=jnp.float32)
    hidden_state = (tokens.astype(jnp.float32) + attn_out).astype(jnp.bfloat16)
    normed_ffn = rms_scale(hidden_state.astype(jnp.float32), g_ffn).astype(jnp.bfloat16)
    shared_gate = jnp.dot(normed_ffn, w_shared_gate, preferred_element_type=jnp.float32)
    shared_up = jnp.dot(normed_ffn, w_shared_up, preferred_element_type=jnp.float32)
    shared_hidden = (jax.nn.silu(shared_gate) * shared_up).astype(jnp.bfloat16)
    shared_out = jnp.dot(shared_hidden, w_shared_down, preferred_element_type=jnp.float32)
    expert_count = w_expert_gate.shape[0]
    most_rows = N_EP * N_TP * CAP
    half_width = EFF // N_TP
    padded = jnp.concatenate([normed_ffn, jnp.zeros((1, D), jnp.bfloat16)], axis=0)

    def per_expert(routed_sum, expert):
        names_it = expert_ids == expert
        weight = lax.optimization_barrier(jnp.sum(jnp.where(names_it, route_weights, 0.0), axis=1))
        weight_pad = jnp.concatenate([weight, jnp.zeros((1,), jnp.float32)])
        picked = jnp.nonzero(jnp.any(names_it, axis=1), size=most_rows, fill_value=row_count)[0].astype(jnp.int32)
        inputs = padded[picked]
        gate_value = jnp.dot(inputs, w_expert_gate[expert], preferred_element_type=jnp.float32)
        up_value = jnp.dot(inputs, w_expert_up[expert], preferred_element_type=jnp.float32)
        hidden = (jax.nn.silu(gate_value) * up_value).astype(jnp.bfloat16)
        part_total = jnp.zeros((most_rows, D), jnp.float32)
        for part_index in range(N_TP):
            part_piece = jnp.dot(hidden[:, part_index * half_width:(part_index + 1) * half_width], w_expert_down[expert, part_index * half_width:(part_index + 1) * half_width], preferred_element_type=jnp.float32)
            part_total = part_total + lax.optimization_barrier(part_piece.astype(jnp.bfloat16)).astype(jnp.float32)
        expert_out = lax.optimization_barrier(part_total.astype(jnp.bfloat16)).astype(jnp.float32)
        routed_sum = routed_sum.at[picked].add(weight_pad[picked][:, None] * expert_out)
        return (routed_sum, None)
    routed, _ = lax.scan(per_expert, jnp.zeros((row_count + 1, D), jnp.float32), jnp.arange(expert_count, dtype=jnp.int32))
    mixed_out = (hidden_state.astype(jnp.float32) + routed[:row_count] + shared_out).astype(jnp.bfloat16)
    return (mixed_out, new_entry)
```

```python
import functools

import jax
import jax.numpy as jnp
from jax import lax
from jax.experimental import pallas as pl
from jax.experimental.pallas import tpu as pltpu
from jax.sharding import PartitionSpec as P

HEADS = 16
NOPE = 64
ROPE = 32
VDIM = 64
CAP = 4
GROUP = 8

norm_eps = 1e-06
masked_score = -1e30
F32 = jnp.float32
BF16 = jnp.bfloat16
MESH = pl.DeviceIdType.MESH


def nn(a, b):
    return jnp.dot(a, b, preferred_element_type=F32)


def nt(a, b):
    return lax.dot_general(a, b, (((1,), (1,)), ((), ())), preferred_element_type=F32)


def iota(shape, axis):
    return lax.broadcasted_iota(jnp.int32, shape, axis)


def rms(values, gain):
    mean_square = jnp.mean(values * values, axis=-1, keepdims=True)
    return values * lax.rsqrt(mean_square + norm_eps) * gain


def silu(v):
    return v / (1.0 + jnp.exp(-v))


def onehot(cond):
    return jnp.where(cond, 1.0, 0.0).astype(BF16)


def step_kernel(ep_size, tp_size, names, *refs):
    count = len(names)
    hbm = dict(zip(names, refs[:count]))
    out_ref, entry_ref = refs[count : count + 2]
    refs = refs[count + 2 :]
    vmem = dict(zip(names, refs[:count]))
    (
        ql_ref,
        qr_ref,
        mix_ref,
        spread_ref,
        outbox,
        inbox,
        ret_out,
        ret_in,
        in_sem,
        cache_sem,
        rope_sem,
        swap_send,
        swap_recv,
        out_send,
        out_recv,
        back_send,
        back_recv,
    ) = refs[count:]
    rows, width = hbm["tokens"].shape
    length = hbm["latent_cache"].shape[1]
    own_experts = vmem["w_expert_gate"].shape[1]
    devices = ep_size * tp_size
    block = own_experts * CAP
    slots = devices * block
    ep = lax.axis_index("ep")
    tp = lax.axis_index("tp")
    me = ep * tp_size + tp
    paired = devices & (devices - 1) == 0

    def flip(d, s):
        total = 0
        for k in range(devices.bit_length() - 1):
            total = total + ((d // (1 << k) + s // (1 << k)) % 2) * (1 << k)
        return total

    def target(s):
        return flip(me, s) if paired else lax.rem(me + s, devices)

    def source(s):
        return flip(me, s) if paired else lax.rem(me + devices - s, devices)

    def ident(d):
        return {"ep": d // tp_size, "tp": d % tp_size}

    def each(steps, visit):
        if len(steps) <= 16:
            for s in steps:
                visit(s)
        else:
            low = min(steps)
            high = max(steps)

            @pl.loop(0, high - low + 1)
            def _(i):
                visit(high - i)

    expert_names = ("w_expert_gate", "w_expert_up", "w_expert_down")

    def load(name):
        i = names.index(name)
        if name in expert_names:
            src = hbm[name].at[pl.ds(tp * own_experts, own_experts)]
            return pltpu.make_async_copy(src, vmem[name].at[tp], in_sem.at[i])
        return pltpu.make_async_copy(hbm[name], vmem[name], in_sem.at[i])

    def cache_copies(g):
        part = pl.ds(g * GROUP, GROUP)
        return (
            pltpu.make_async_copy(
                hbm["latent_cache"].at[part], vmem["latent_cache"].at[part], cache_sem.at[g]
            ),
            pltpu.make_async_copy(
                hbm["rope_cache"].at[part], vmem["rope_cache"].at[part], rope_sem.at[g]
            ),
        )

    groups = rows // GROUP
    first = ("tokens", "g_attn", "w_query_down", "g_query", "lengths", "expert_ids")
    second = ("w_query", "w_query_rope", "w_key_up")
    late = (
        "w_value_up", "w_out", "g_ffn", "w_shared_gate", "w_shared_up", "w_shared_down",
        "route_weights", "w_latent_down", "g_latent", "w_rope_key",
    ) + expert_names
    for name in first + second:
        load(name).start()
    barrier = pltpu.get_barrier_semaphore()

    @pl.loop(1, devices)
    def _(i):
        pl.semaphore_signal(
            barrier, inc=1, device_id=ident(lax.rem(me + i, devices)), device_id_type=MESH
        )

    @pl.loop(0, groups)
    def _(g):
        for copy in cache_copies(g):
            copy.start()

    for name in late:
        load(name).start()

    def ready(name):
        load(name).wait()
        return vmem[name]
    for name in first:
        load(name).wait()
    lens = vmem["lengths"]
    ids = vmem["expert_ids"][...]
    slot = iota((slots, rows), 0)
    step = lax.div(slot, block)
    if paired:
        owner = lax.bitwise_xor(step, jnp.zeros_like(step) + me)
    else:
        owner = lax.rem(step + me, devices)
    slot_expert = owner * own_experts + lax.div(lax.rem(slot, block), CAP)
    named = jnp.zeros((slots, rows), F32)
    for k in range(ids.shape[0]):
        named = jnp.where(slot_expert == ids[k : k + 1, :], 1.0, named)
    before = onehot(iota((rows, rows), 0) < iota((rows, rows), 1))
    rank = nn(named.astype(BF16), before)
    taken = jnp.logical_and(named > 0.5, rank == (slot & (CAP - 1)).astype(F32))
    spread_ref[...] = onehot(taken)

    row_id = iota((rows, 128), 0)
    position = jnp.zeros((rows, 128), F32)
    for s in range(rows):
        position = jnp.where(row_id == s, lens[s].astype(F32), position)
    lane = iota((rows, 128), 1)
    half = ROPE // 2
    frequency = jnp.exp((lane & (half - 1)).astype(F32) * (-9.210340371976184 / half))
    angle = position * frequency
    cosine = jnp.cos(angle)
    sine = jnp.sin(angle)
    sine = jnp.where((lane & (ROPE - 1)) < half, -sine, sine)

    tokens = vmem["tokens"][...].astype(F32)
    normed = rms(tokens, vmem["g_attn"][...]).astype(BF16)
    query_low = rms(nn(normed, vmem["w_query_down"][...]), vmem["g_query"][...]).astype(BF16)
    query = nn(query_low, ready("w_query")[...]).astype(BF16)
    turn = nn(query_low, ready("w_query_rope")[...])
    rope_width = turn.shape[1]
    rope_lane = iota((rows, rope_width), 1)
    swapped = jnp.where(
        (rope_lane & (ROPE - 1)) < half,
        pltpu.roll(turn, rope_width - half, 1),
        pltpu.roll(turn, half, 1),
    )
    tiles = rope_width // 128
    turned = (
        turn * jnp.concatenate([cosine] * tiles, axis=1)
        + swapped * jnp.concatenate([sine] * tiles, axis=1)
    ).astype(BF16)
    pairs = rows * HEADS
    repeat = onehot(lax.shift_right_logical(iota((pairs, rows), 0), 4) == iota((pairs, rows), 1))

    def head_mask(columns, shift):
        head = iota((pairs, columns), 0) & (HEADS - 1)
        return head == lax.shift_right_logical(iota((pairs, columns), 1), shift)
    nope_mask = head_mask(query.shape[1], 6)
    spread_query = jnp.where(nope_mask, nn(repeat, query), 0.0).astype(BF16)
    ql_ref[...] = nt(spread_query, ready("w_key_up")[...]).astype(BF16)
    spread_turn = jnp.where(head_mask(rope_width, 5), nn(repeat, turned), 0.0).astype(BF16)
    fold = onehot(
        (iota((rope_width, ROPE), 0) & (ROPE - 1)) == iota((rope_width, ROPE), 1)
    )
    qr_ref[...] = nn(spread_turn, fold).astype(BF16)

    swaps = []
    for p in range(1, tp_size):
        peer = lax.rem(tp + p, tp_size)
        for i, name in enumerate(expert_names):
            swaps.append(
                pltpu.make_async_remote_copy(
                    src_ref=hbm[name].at[pl.ds(peer * own_experts, own_experts)],
                    dst_ref=vmem[name].at[tp],
                    send_sem=swap_send.at[i, p],
                    recv_sem=swap_recv.at[i, p],
                    device_id={"tp": peer},
                    device_id_type=MESH,
                )
            )

    scale = (NOPE + ROPE) ** (-0.5)
    time_lane = iota((HEADS, length), 1)

    def attend(g):
        for copy in cache_copies(g):
            copy.wait()
        parts = []
        scored = []
        for j in range(GROUP):
            s = g * GROUP + j
            part = pl.ds(pl.multiple_of(s * HEADS, HEADS), HEADS)
            parts.append((s, part))
            scores = nt(ql_ref[part, :], vmem["latent_cache"][s])
            scored.append(scores + nn(qr_ref[part, :], vmem["rope_cache"][s]))
        soft = []
        for (s, part), scores in zip(parts, scored):
            live = time_lane < lens[s]
            scores = jnp.where(live, scores * scale, masked_score)
            top = jnp.max(scores, axis=1, keepdims=True)
            weights = jnp.where(live, jnp.exp(scores - top), 0.0)
            soft.append((weights.astype(BF16), jnp.sum(weights, axis=1, keepdims=True)))
        for (s, part), (weights, total) in zip(parts, soft):
            mixed = nn(weights, vmem["latent_cache"][s])
            mix_ref[part, :] = (mixed / total).astype(BF16)

    @pl.loop(0, groups - 1)
    def _(g):
        attend(g)

    pl.semaphore_wait(barrier, devices - 1)
    for copy in swaps:
        copy.start()

    attend(groups - 1)
    heads_all = nn(mix_ref[...], ready("w_value_up")[...])
    heads_all = jnp.where(head_mask(heads_all.shape[1], 6), heads_all, 0.0).astype(BF16)
    gather = onehot(iota((rows, pairs), 0) == lax.shift_right_logical(iota((rows, pairs), 1), 4))
    value_heads = nn(gather, heads_all).astype(BF16)
    hidden = (tokens + nn(value_heads, ready("w_out")[...])).astype(BF16).astype(F32)
    normed_ffn = rms(hidden, ready("g_ffn")[...]).astype(BF16)
    box = nn(spread_ref[...], normed_ffn).astype(BF16)
    for s in range(devices):
        place = inbox if s == 0 else outbox
        place[s] = box[s * block : (s + 1) * block, :]

    def message(src, dst, send, recv, s, d):
        return pltpu.make_async_remote_copy(
            src_ref=src.at[s],
            dst_ref=dst.at[s],
            send_sem=send.at[s],
            recv_sem=recv.at[s],
            device_id=ident(d),
            device_id_type=MESH,
        )

    def there(s):
        return message(outbox, inbox, out_send, out_recv, s, target(s))

    def back(s):
        return message(ret_out, ret_in, back_send, back_recv, s, source(s))
    each(range(devices - 1, 0, -1), lambda s: there(s).start())
    shared_gate = nn(normed_ffn, ready("w_shared_gate")[...])
    shared_up = nn(normed_ffn, ready("w_shared_up")[...])
    shared_hidden = (silu(shared_gate) * shared_up).astype(BF16)
    base = hidden + nn(shared_hidden, ready("w_shared_down")[...])
    gain_latent = ready("g_latent")[...]
    latent_new = rms(nn(normed, ready("w_latent_down")[...]), gain_latent)
    key = nt(normed, ready("w_rope_key")[...])
    swapped = jnp.concatenate([key[:, half:], key[:, :half]], axis=1)
    key_new = key * cosine[:, :ROPE] + swapped * sine[:, :ROPE]
    kvl = latent_new.shape[1]
    entry_ref[:, 0:kvl] = latent_new.astype(BF16)
    entry_ref[:, kvl : kvl + ROPE] = key_new.astype(BF16)
    route = ready("route_weights")[...]
    slot_weight = jnp.zeros((slots, rows), F32)
    for k in range(ids.shape[0]):
        hit = slot_expert == ids[k : k + 1, :]
        slot_weight = jnp.where(hit, route[k : k + 1, :], slot_weight)
    slot_weight = jnp.where(spread_ref[...].astype(F32) > 0.5, slot_weight, 0.0)
    high = slot_weight.astype(BF16)
    low = (slot_weight - high.astype(F32)).astype(BF16)
    eye = onehot(iota((rows, rows), 0) == iota((rows, rows), 1))
    weight_high = nt(eye, high).astype(BF16)
    weight_low = nt(eye, low).astype(BF16)
    for name in expert_names:
        load(name).wait()
    for copy in swaps:
        copy.wait()
    gates, ups, downs = (vmem[name] for name in expert_names)

    def serve(steps):
        for e in range(own_experts):
            x = jnp.concatenate(
                [inbox[s, e * CAP : (e + 1) * CAP, :] for s in steps], axis=0
            )
            total = jnp.zeros((len(steps) * CAP, width), F32)
            for t in range(tp_size):
                unit = (silu(nn(x, gates[t, e])) * nn(x, ups[t, e])).astype(BF16)
                total = total + nn(unit, downs[t, e]).astype(BF16).astype(F32)
            total = total.astype(BF16)
            for i, s in enumerate(steps):
                place = ret_in if s == 0 else ret_out
                place[s, e * CAP : (e + 1) * CAP, :] = total[i * CAP : (i + 1) * CAP, :]

    quarter = max(devices // 4, 1)
    chunks = [range(i, min(i + quarter, devices)) for i in range(0, devices, quarter)]
    chunks = chunks[:1] + chunks[:0:-1]
    for chunk in chunks:
        remote = range(max(chunk[-1], 0), max(chunk[0], 1) - 1, -1)
        each(remote, lambda s: there(s).wait_recv())
        serve(chunk)
        each(remote, lambda s: back(s).start())
    each(range(devices - 1, 0, -1), lambda s: there(s).wait_send())
    each(range(devices - 1, 0, -1), lambda s: back(s).wait_send())
    each(range(devices - 1, 0, -1), lambda s: back(s).wait_recv())
    returned = jnp.concatenate([ret_in[s] for s in range(devices)], axis=0)
    both = nn(weight_high, returned) + nn(weight_low, returned)
    out_ref[...] = (base + both).astype(BF16)


NAMES = (
    "tokens", "latent_cache", "rope_cache", "expert_ids", "route_weights", "g_attn",
    "w_query_down", "g_query", "w_latent_down", "g_latent", "w_rope_key", "w_query",
    "w_query_rope", "w_key_up", "w_value_up", "w_out", "g_ffn", "w_expert_gate",
    "w_expert_up", "w_expert_down", "w_shared_gate", "w_shared_up", "w_shared_down",
    "lengths",
)


def local(tokens, latent_cache, rope_cache, lengths, expert_ids, route_weights, *weights):
    named = dict(
        zip(NAMES, (tokens, latent_cache, rope_cache, expert_ids, route_weights) + weights + (lengths,))
    )
    for name in ("g_attn", "g_query", "g_latent", "g_ffn"):
        named[name] = named[name].reshape(1, -1)
    named["rope_cache"] = jnp.swapaxes(rope_cache, 1, 2)
    for name in ("expert_ids", "route_weights", "w_rope_key"):
        named[name] = named[name].T
    ep_size = lax.axis_size("ep")
    tp_size = lax.axis_size("tp")
    devices = ep_size * tp_size
    own = named["w_expert_gate"].shape[0] // tp_size
    rows, width = tokens.shape
    pairs = rows * HEADS
    kvl = latent_cache.shape[2]
    slots = devices * own * CAP

    def holder(name):
        shape = named[name].shape
        if name.startswith("w_expert"):
            shape = (tp_size, own) + shape[1:]
        if name == "lengths":
            return pltpu.SMEM(shape, named[name].dtype)
        return pltpu.VMEM(shape, named[name].dtype)

    box = pltpu.VMEM((devices, own * CAP, width), BF16)
    dma = pltpu.SemaphoreType.DMA
    return pl.pallas_call(
        functools.partial(step_kernel, ep_size, tp_size, NAMES),
        out_shape=(
            pltpu.VMEM((rows, width), BF16),
            pltpu.VMEM((rows, kvl + ROPE), BF16),
        ),
        in_specs=[pl.BlockSpec(memory_space=pl.ANY)] * len(NAMES),
        out_specs=(pl.BlockSpec(memory_space=pltpu.VMEM),) * 2,
        scratch_shapes=[holder(name) for name in NAMES]
        + [
            pltpu.VMEM((pairs, kvl), BF16),
            pltpu.VMEM((pairs, ROPE), BF16),
            pltpu.VMEM((pairs, kvl), BF16),
            pltpu.VMEM((slots, rows), BF16),
            box,
            box,
            box,
            box,
            dma((len(NAMES),)),
            dma((rows // GROUP,)),
            dma((rows // GROUP,)),
            dma((3, tp_size)),
            dma((3, tp_size)),
            dma((devices,)),
            dma((devices,)),
            dma((devices,)),
            dma((devices,)),
        ],
        compiler_params=pltpu.CompilerParams(
            collective_id=0, has_side_effects=True, vmem_limit_bytes=60 * 1024 * 1024
        ),
        name="decode_step",
    )(*[named[name] for name in NAMES])


def solution(mesh):
    split = ("grp", "ep", "tp")
    in_specs = (
        (P(split, None), P(split, None, None), P(split, None, None), P(split))
        + (P(split, None), P(split, None))
        + (P(),) * 12
        + (P("ep", None, "tp"), P("ep", None, "tp"), P("ep", "tp", None))
        + (P(),) * 3
    )
    out_specs = (P(split, None), P(split, None))
    return jax.shard_map(local, mesh=mesh, in_specs=in_specs, out_specs=out_specs, check_vma=False)
```

```python
import functools

import jax
import jax.numpy as jnp
from jax import lax
from jax.experimental import pallas as pl
from jax.experimental.pallas import tpu as pltpu
from jax.sharding import PartitionSpec as P

HEADS = 16
NOPE = 64
ROPE = 32
VDIM = 64
CAP = 4
GROUP = 4

norm_eps = 1e-06
masked_score = -1e30
F32 = jnp.float32
BF16 = jnp.bfloat16
MESH = pl.DeviceIdType.MESH


def nn(a, b):
    return jnp.dot(a, b, preferred_element_type=F32)


def nt(a, b):
    return lax.dot_general(a, b, (((1,), (1,)), ((), ())), preferred_element_type=F32)


def iota(shape, axis):
    return lax.broadcasted_iota(jnp.int32, shape, axis)


def rms(values, gain):
    mean_square = jnp.mean(values * values, axis=-1, keepdims=True)
    return values * lax.rsqrt(mean_square + norm_eps) * gain


def silu(v):
    return v / (1.0 + jnp.exp(-v))


def onehot(cond):
    return jnp.where(cond, 1.0, 0.0).astype(BF16)


def step_kernel(ep_size, tp_size, names, *refs):
    count = len(names)
    hbm = dict(zip(names, refs[:count]))
    out_ref, entry_ref = refs[count : count + 2]
    refs = refs[count + 2 :]
    vmem = dict(zip(names, refs[:count]))
    (
        ql_ref,
        qr_ref,
        mix_ref,
        turned_ref,
        spread_ref,
        outbox,
        inbox,
        ret_out,
        ret_in,
        in_sem,
        cache_sem,
        rope_sem,
        swap_send,
        swap_recv,
        out_send,
        out_recv,
        back_send,
        back_recv,
    ) = refs[count:]
    rows, width = hbm["tokens"].shape
    length = hbm["latent_cache"].shape[1]
    own_experts = vmem["w_expert_gate"].shape[0]
    devices = ep_size * tp_size
    block = own_experts * CAP
    slots = devices * block
    ep = lax.axis_index("ep")
    tp = lax.axis_index("tp")
    me = ep * tp_size + tp
    planes = 4 if devices % 4 == 0 else 1
    crew = devices // planes
    plane = me // crew
    seat = me % crew

    def across(k):
        total = 0
        for b in range(planes.bit_length() - 1):
            total = total + ((plane // (1 << b) + (k >> b)) % 2) * (1 << b)
        return total

    def ident(d):
        return {"ep": d // tp_size, "tp": d % tp_size}

    def each(low, high, visit):
        if high - low <= 16:
            for i in range(low, high):
                visit(i)
        else:
            pl.loop(low, high)(visit)

    expert_names = ("w_expert_gate", "w_expert_up", "w_expert_down")

    def shard(name, owner):
        axis = 1 if name == "w_expert_down" else 2
        units = hbm[name].shape[axis]
        part = pl.ds(pl.multiple_of(owner * units, units), units)
        if axis == 1:
            return vmem[name].at[:, part, :]
        return vmem[name].at[:, :, part]

    def load(name):
        i = names.index(name)
        if name in expert_names:
            src = hbm[name].at[pl.ds(tp * own_experts, own_experts)]
            return pltpu.make_async_copy(src, shard(name, tp), in_sem.at[i])
        return pltpu.make_async_copy(hbm[name], vmem[name], in_sem.at[i])

    def cache_copies(g):
        part = pl.ds(g * GROUP, GROUP)
        return (
            pltpu.make_async_copy(
                hbm["latent_cache"].at[part], vmem["latent_cache"].at[part], cache_sem.at[g]
            ),
            pltpu.make_async_copy(
                hbm["rope_cache"].at[part], vmem["rope_cache"].at[part], rope_sem.at[g]
            ),
        )

    groups = rows // GROUP
    first = ("tokens", "g_attn", "w_query_down", "g_query", "lengths", "expert_ids")
    second = ("w_query", "w_query_rope", "w_key_up")
    third = ("w_value_up", "w_out", "g_ffn")
    late = (
        "w_shared_gate", "w_shared_up", "w_shared_down", "route_weights", "w_latent_down",
        "g_latent", "w_rope_key",
    ) + expert_names

    def begin(g):
        if g < groups:
            for copy in cache_copies(g):
                copy.start()

    for name in first + second:
        load(name).start()
    begin(0)
    barrier = pltpu.get_barrier_semaphore()

    @pl.loop(1, devices)
    def _(i):
        pl.semaphore_signal(
            barrier, inc=1, device_id=ident(lax.rem(me + i, devices)), device_id_type=MESH
        )

    def ready(name):
        load(name).wait()
        return vmem[name]
    for name in first:
        load(name).wait()
    begin(1)
    lens = vmem["lengths"]
    ids = vmem["expert_ids"][...]
    slot = iota((slots, rows), 0)
    step = lax.div(slot, block)
    owner = lax.div(step, crew) * crew + lax.rem(lax.rem(step, crew) + seat, crew)
    slot_expert = owner * own_experts + lax.div(lax.rem(slot, block), CAP)
    named = jnp.zeros((slots, rows), F32)
    for k in range(ids.shape[0]):
        named = jnp.where(slot_expert == ids[k : k + 1, :], 1.0, named)
    before = onehot(iota((rows, rows), 0) < iota((rows, rows), 1))
    rank = nn(named.astype(BF16), before)
    taken = jnp.logical_and(named > 0.5, rank == (slot & (CAP - 1)).astype(F32))
    spread_ref[...] = onehot(taken)

    row_id = iota((rows, 128), 0)
    position = jnp.zeros((rows, 128), F32)
    for s in range(rows):
        position = jnp.where(row_id == s, lens[s].astype(F32), position)
    lane = iota((rows, 128), 1)
    half = ROPE // 2
    frequency = jnp.exp((lane & (half - 1)).astype(F32) * (-9.210340371976184 / half))
    angle = position * frequency
    cosine = jnp.cos(angle)
    sine = jnp.sin(angle)
    sine = jnp.where((lane & (ROPE - 1)) < half, -sine, sine)

    tokens = vmem["tokens"][...].astype(F32)
    normed = rms(tokens, vmem["g_attn"][...]).astype(BF16)
    query_low = rms(nn(normed, vmem["w_query_down"][...]), vmem["g_query"][...]).astype(BF16)
    begin(2)
    query = nn(query_low, ready("w_query")[...])
    turn = nn(query_low, ready("w_query_rope")[...])
    rope_width = turn.shape[1]
    rope_lane = iota((rows, rope_width), 1)
    swapped = jnp.where(
        (rope_lane & (ROPE - 1)) < half,
        pltpu.roll(turn, rope_width - half, 1),
        pltpu.roll(turn, half, 1),
    )
    tiles = rope_width // 128
    turned = (
        turn * jnp.concatenate([cosine] * tiles, axis=1)
        + swapped * jnp.concatenate([sine] * tiles, axis=1)
    )
    for h in range(HEADS):
        tile, place = divmod(h * ROPE, 128)
        lanes = turned[:, tile * 128 : (tile + 1) * 128]
        if place:
            lanes = pltpu.roll(lanes, 128 - place, 1)
        qr_ref[h * rows : (h + 1) * rows, :] = lanes
    def put_wide(ref, part, value):
        for t in range(ref.shape[0]):
            ref[t, part, :] = value[:, t * 128 : (t + 1) * 128]

    def get_wide(ref, part):
        return jnp.concatenate([ref[t, part, :] for t in range(ref.shape[0])], axis=1)

    span = 256
    quad = span // NOPE
    quad_lane = iota((rows, span), 1) // NOPE
    w_key_up = ready("w_key_up")
    for g in range(3, groups):
        begin(g)
    for copy in cache_copies(0):
        copy.wait()

    def turn_keys(s):
        turned_ref[s % (2 * GROUP)] = vmem["latent_cache"][s].T

    for name in third:
        load(name).start()
    for s in range(GROUP):
        turn_keys(s)
    for n in range(HEADS // quad):
        piece = query[:, n * span : (n + 1) * span]
        spread_query = jnp.concatenate(
            [jnp.where(quad_lane == j, piece, 0.0) for j in range(quad)], axis=0
        )
        put_wide(
            ql_ref,
            pl.ds(n * quad * rows, quad * rows),
            nt(spread_query.astype(BF16), w_key_up[:, n * span : (n + 1) * span]),
        )

    swaps = []
    for p in range(1, tp_size):
        peer = lax.rem(tp + p, tp_size)
        for i, name in enumerate(expert_names):
            swaps.append(
                pltpu.make_async_remote_copy(
                    src_ref=hbm[name].at[pl.ds(peer * own_experts, own_experts)],
                    dst_ref=shard(name, tp),
                    send_sem=swap_send.at[i, p],
                    recv_sem=swap_recv.at[i, p],
                    device_id={"tp": peer},
                    device_id_type=MESH,
                )
            )

    scale = (NOPE + ROPE) ** (-0.5)
    time_lane = iota((HEADS, length), 1)

    def head_rows(s):
        return pl.ds(s, HEADS, stride=rows)

    def score(s):
        query_latent = get_wide(ql_ref, head_rows(s)).astype(BF16)
        query_rope = qr_ref[head_rows(s), :][:, 0:ROPE].astype(BF16)
        found = nn(query_latent, turned_ref[s % (2 * GROUP)])
        return found + nn(query_rope, vmem["rope_cache"][s])

    def soften(s, scores):
        live = time_lane < lens[s]
        scores = jnp.where(live, scores * scale, masked_score)
        top = jnp.max(scores, axis=1, keepdims=True)
        weights = jnp.where(live, jnp.exp(scores - top), 0.0)
        return weights.astype(BF16), jnp.sum(weights, axis=1, keepdims=True)

    def mix(s, weights, total):
        mixed = nn(weights, vmem["latent_cache"][s])
        put_wide(mix_ref, head_rows(s), mixed / total)

    members = [range(g * GROUP, (g + 1) * GROUP) for g in range(groups)]
    scored = []
    for g in range(groups + 1):
        if g + 1 < groups:
            for copy in cache_copies(g + 1):
                copy.wait()
        if g == 0:
            for name in late:
                load(name).start()
        if g == groups - 1:
            pl.semaphore_wait(barrier, devices - 1)
            for copy in swaps:
                copy.start()
        if g == groups:
            for name in third:
                load(name).wait()
        soft = []
        if g > 0:
            soft = [soften(s, scores) for s, scores in zip(members[g - 1], scored)]
        if g < groups:
            scored = [score(s) for s in members[g]]
        if g + 1 < groups:
            for s in members[g + 1]:
                turn_keys(s)
        for s, (weights, total) in zip(members[g - 1], soft):
            mix(s, weights, total)
    value_pieces = []
    for n in range(HEADS // quad):
        part = get_wide(mix_ref, pl.ds(n * quad * rows, quad * rows)).astype(BF16)
        part = nn(part, vmem["w_value_up"][:, n * span : (n + 1) * span])
        piece = part[0:rows]
        for j in range(1, quad):
            piece = jnp.where(quad_lane == j, part[j * rows : (j + 1) * rows], piece)
        value_pieces.append(piece.astype(BF16))
    value_heads = jnp.concatenate(value_pieces, axis=1)
    hidden = (tokens + nn(value_heads, vmem["w_out"][...])).astype(BF16).astype(F32)
    normed_ffn = rms(hidden, vmem["g_ffn"][...]).astype(BF16)
    box = nn(spread_ref[...], normed_ffn).astype(BF16)
    for s in range(devices):
        outbox[s] = box[s * block : (s + 1) * block, :]
    inbox[plane * crew] = outbox[plane * crew]

    def message(src, dst, send, recv, p, i, d):
        return pltpu.make_async_remote_copy(
            src_ref=src.at[p * crew + i],
            dst_ref=dst.at[plane * crew + i],
            send_sem=send.at[p * crew + i],
            recv_sem=recv.at[plane * crew + i],
            device_id=ident(p * crew + d),
            device_id_type=MESH,
        )

    def there(p, i):
        return message(outbox, inbox, out_send, out_recv, p, i, lax.rem(seat + i, crew))

    def back(p, i):
        return message(ret_out, ret_in, back_send, back_recv, p, i, lax.rem(seat + crew - i, crew))

    def arrival(dst, recv, p, i):
        spot = dst.at[p * crew + i]
        return pltpu.make_async_remote_copy(
            src_ref=spot,
            dst_ref=spot,
            send_sem=out_send.at[p * crew + i],
            recv_sem=recv.at[p * crew + i],
            device_id=ident(me),
            device_id_type=MESH,
        )

    def peers(visit):
        for k in range(planes - 1, -1, -1):
            p = across(k)
            each(0 if k else 1, crew, lambda i, p=p: visit(p, i))
    peers(lambda p, i: there(p, i).start())
    shared_gate = nn(normed_ffn, ready("w_shared_gate")[...])
    shared_up = nn(normed_ffn, ready("w_shared_up")[...])
    shared_hidden = (silu(shared_gate) * shared_up).astype(BF16)
    base = hidden + nn(shared_hidden, ready("w_shared_down")[...])
    gain_latent = ready("g_latent")[...]
    latent_new = rms(nn(normed, ready("w_latent_down")[...]), gain_latent)
    key = nt(normed, ready("w_rope_key")[...])
    swapped = jnp.concatenate([key[:, half:], key[:, :half]], axis=1)
    key_new = key * cosine[:, :ROPE] + swapped * sine[:, :ROPE]
    kvl = latent_new.shape[1]
    entry_ref[:, 0:kvl] = latent_new.astype(BF16)
    entry_ref[:, kvl : kvl + ROPE] = key_new.astype(BF16)
    route = ready("route_weights")[...]
    slot_weight = jnp.zeros((slots, rows), F32)
    for k in range(ids.shape[0]):
        hit = slot_expert == ids[k : k + 1, :]
        slot_weight = jnp.where(hit, route[k : k + 1, :], slot_weight)
    slot_weight = jnp.where(spread_ref[...].astype(F32) > 0.5, slot_weight, 0.0)
    high = slot_weight.astype(BF16)
    low = (slot_weight - high.astype(F32)).astype(BF16)
    eye = onehot(iota((rows, rows), 0) == iota((rows, rows), 1))
    weight_high = nt(eye, high).astype(BF16)
    weight_low = nt(eye, low).astype(BF16)
    for name in expert_names:
        load(name).wait()
    for copy in swaps:
        copy.wait()
    gates, ups, downs = (vmem[name] for name in expert_names)

    def serve(p):
        steps = range(p * crew, (p + 1) * crew)
        for e in range(own_experts):
            x = jnp.concatenate(
                [inbox[s, e * CAP : (e + 1) * CAP, :] for s in steps], axis=0
            )
            unit = (silu(nn(x, gates[e])) * nn(x, ups[e])).astype(BF16)
            total = nn(unit, downs[e]).astype(BF16)
            for i, s in enumerate(steps):
                ret_out[s, e * CAP : (e + 1) * CAP, :] = total[i * CAP : (i + 1) * CAP, :]

    for p in range(planes):
        each(1, crew, lambda i: arrival(inbox, out_recv, p, i).wait_recv())

        @pl.when(plane != p)
        def _():
            arrival(inbox, out_recv, p, 0).wait_recv()
        serve(p)
        each(1, crew, lambda i: back(p, i).start())

        @pl.when(plane != p)
        def _():
            back(p, 0).start()

    ret_in[plane * crew] = ret_out[plane * crew]
    peers(lambda p, i: there(p, i).wait_send())
    peers(lambda p, i: back(p, i).wait_send())
    peers(lambda p, i: arrival(ret_in, back_recv, p, i).wait_recv())
    returned = jnp.concatenate([ret_in[s] for s in range(devices)], axis=0)
    both = nn(weight_high, returned) + nn(weight_low, returned)
    out_ref[...] = (base + both).astype(BF16)


NAMES = (
    "tokens", "latent_cache", "rope_cache", "expert_ids", "route_weights", "g_attn",
    "w_query_down", "g_query", "w_latent_down", "g_latent", "w_rope_key", "w_query",
    "w_query_rope", "w_key_up", "w_value_up", "w_out", "g_ffn", "w_expert_gate",
    "w_expert_up", "w_expert_down", "w_shared_gate", "w_shared_up", "w_shared_down",
    "lengths",
)


def local(tokens, latent_cache, rope_cache, lengths, expert_ids, route_weights, *weights):
    named = dict(
        zip(NAMES, (tokens, latent_cache, rope_cache, expert_ids, route_weights) + weights + (lengths,))
    )
    for name in ("g_attn", "g_query", "g_latent", "g_ffn"):
        named[name] = named[name].reshape(1, -1)
    named["rope_cache"] = jnp.swapaxes(rope_cache, 1, 2)
    for name in ("expert_ids", "route_weights", "w_rope_key"):
        named[name] = named[name].T
    ep_size = lax.axis_size("ep")
    tp_size = lax.axis_size("tp")
    devices = ep_size * tp_size
    own = named["w_expert_gate"].shape[0] // tp_size
    rows, width = tokens.shape
    pairs = rows * HEADS
    length, kvl = latent_cache.shape[1:]
    slots = devices * own * CAP

    def holder(name):
        shape = named[name].shape
        if name.startswith("w_expert"):
            axis = 1 if name == "w_expert_down" else 2
            shape = (own,) + tuple(
                n * tp_size if i == axis else n for i, n in enumerate(shape) if i
            )
        if name == "lengths":
            return pltpu.SMEM(shape, named[name].dtype)
        return pltpu.VMEM(shape, named[name].dtype)

    box = pltpu.VMEM((devices, own * CAP, width), BF16)
    dma = pltpu.SemaphoreType.DMA
    return pl.pallas_call(
        functools.partial(step_kernel, ep_size, tp_size, NAMES),
        out_shape=(
            pltpu.VMEM((rows, width), BF16),
            pltpu.VMEM((rows, kvl + ROPE), BF16),
        ),
        in_specs=[pl.BlockSpec(memory_space=pl.ANY)] * len(NAMES),
        out_specs=(pl.BlockSpec(memory_space=pltpu.VMEM),) * 2,
        scratch_shapes=[holder(name) for name in NAMES]
        + [
            pltpu.VMEM((kvl // 128, pairs, 128), F32),
            pltpu.VMEM((pairs, 128), F32),
            pltpu.VMEM((kvl // 128, pairs, 128), F32),
            pltpu.VMEM((2 * GROUP, kvl, length), BF16),
            pltpu.VMEM((slots, rows), BF16),
            box,
            box,
            box,
            box,
            dma((len(NAMES),)),
            dma((rows // GROUP,)),
            dma((rows // GROUP,)),
            dma((3, tp_size)),
            dma((3, tp_size)),
            dma((devices,)),
            dma((devices,)),
            dma((devices,)),
            dma((devices,)),
        ],
        compiler_params=pltpu.CompilerParams(
            collective_id=0, has_side_effects=True, vmem_limit_bytes=60 * 1024 * 1024
        ),
        name="decode_step",
    )(*[named[name] for name in NAMES])


def solution(mesh):
    split = ("grp", "ep", "tp")
    in_specs = (
        (P(split, None), P(split, None, None), P(split, None, None), P(split))
        + (P(split, None), P(split, None))
        + (P(),) * 12
        + (P("ep", None, "tp"), P("ep", None, "tp"), P("ep", "tp", None))
        + (P(),) * 3
    )
    out_specs = (P(split, None), P(split, None))
    return jax.shard_map(local, mesh=mesh, in_specs=in_specs, out_specs=out_specs, check_vma=False)
```

```python
import functools
import math

import jax
import jax.numpy as jnp
from jax import lax
from jax.experimental import pallas as pl
from jax.experimental.pallas import tpu as pltpu
from jax.sharding import PartitionSpec as P

HEADS = 16
NOPE = 64
ROPE = 32
VDIM = 64
CAP = 4
GROUP = 4

norm_eps = 1e-06
masked_score = -1e30
F32 = jnp.float32
BF16 = jnp.bfloat16
MESH = pl.DeviceIdType.MESH


def nn(a, b):
    return jnp.dot(a, b, preferred_element_type=F32)


def nt(a, b):
    return lax.dot_general(a, b, (((1,), (1,)), ((), ())), preferred_element_type=F32)


def iota(shape, axis):
    return lax.broadcasted_iota(jnp.int32, shape, axis)


def rms(values, gain):
    mean_square = jnp.mean(values * values, axis=-1, keepdims=True)
    return values * lax.rsqrt(mean_square + norm_eps) * gain


def silu(v):
    return v / (1.0 + jnp.exp(-v))


def onehot(cond):
    return jnp.where(cond, 1.0, 0.0).astype(BF16)


def step_kernel(ep_size, tp_size, names, *refs):
    count = len(names)
    hbm = dict(zip(names, refs[:count]))
    out_ref, entry_ref = refs[count : count + 2]
    refs = refs[count + 2 :]
    vmem = dict(zip(names, refs[:count]))
    (
        ql_ref,
        qr_ref,
        mix_ref,
        turned_ref,
        spread_ref,
        outbox,
        inbox,
        ret_out,
        ret_in,
        small_sem,
        load_sem,
        cache_sem,
        swap_send,
        swap_recv,
        send_sem,
        out_recv,
        back_recv,
    ) = refs[count:]
    rows, width = hbm["tokens"].shape
    length = hbm["latent_cache"].shape[1]
    own_experts = vmem["w_expert_gate"].shape[0]
    devices = ep_size * tp_size
    block = own_experts * CAP
    slots = devices * block
    ep = lax.axis_index("ep")
    tp = lax.axis_index("tp")
    me = ep * tp_size + tp
    planes = 4 if devices % 4 == 0 else 1
    crew = devices // planes
    plane = me // crew
    seat = me % crew

    def across(k):
        total = 0
        for b in range(planes.bit_length() - 1):
            total = total + ((plane // (1 << b) + (k >> b)) % 2) * (1 << b)
        return total

    def ident(d):
        return {"ep": d // tp_size, "tp": d % tp_size}

    def each(low, high, visit):
        if high - low <= 16:
            for i in range(low, high):
                visit(i)
        else:
            pl.loop(low, high)(visit)

    expert_names = ("w_expert_gate", "w_expert_up", "w_expert_down")

    def shard(name, owner):
        axis = 1 if name == "w_expert_down" else 2
        units = hbm[name].shape[axis]
        part = pl.ds(pl.multiple_of(owner * units, units), units)
        if axis == 1:
            return vmem[name].at[:, part, :]
        return vmem[name].at[:, :, part]

    small = (
        "lengths", "expert_ids", "route_weights", "g_attn", "g_query", "g_latent", "g_ffn",
    )
    first = ("tokens", "w_query_down")
    second = ("w_query", "w_query_rope", "w_key_up")
    third = ("w_value_up", "w_out")
    fourth = (
        "w_shared_gate", "w_shared_up", "w_shared_down", "w_latent_down", "w_rope_key",
    )
    batches = (first, second, third, fourth, expert_names)

    def source_of(name):
        if name in expert_names:
            return hbm[name].at[pl.ds(tp * own_experts, own_experts)]
        return hbm[name]

    def load(batch):
        if batch in small:
            sem = small_sem.at[small.index(batch)]
            return pltpu.make_async_copy(hbm[batch], vmem[batch], sem)
        sem = load_sem.at[batches.index(batch)]
        for name in batch:
            place = shard(name, tp) if name in expert_names else vmem[name]
            pltpu.make_async_copy(source_of(name), place, sem).start()

    def size_of(ref):
        return math.prod(ref.shape) * jnp.dtype(ref.dtype).itemsize

    def landed(total, sem):
        cache = hbm["latent_cache"]
        row = cache.shape[2] * 2
        shapes = [
            (n, total // (n * row))
            for n in range(1, rows + 1)
            if total % (16 * n * row) == 0 and total // (n * row) <= length
        ]
        n, depth = shapes[0]
        part = (pl.ds(0, n), pl.ds(0, depth))
        pltpu.make_async_copy(cache.at[part], vmem["latent_cache"].at[part], sem).wait()

    def finish(batch):
        total = sum(size_of(source_of(name)) for name in batch)
        landed(total, load_sem.at[batches.index(batch)])

    def cache_copies(g):
        part = pl.ds(g * GROUP, GROUP)
        return (
            pltpu.make_async_copy(
                hbm["latent_cache"].at[part], vmem["latent_cache"].at[part], cache_sem.at[g]
            ),
            pltpu.make_async_copy(
                hbm["rope_cache"].at[part], vmem["rope_cache"].at[part], cache_sem.at[g]
            ),
        )

    def cache_wait(g):
        part = pl.ds(0, GROUP)
        total = size_of(hbm["latent_cache"].at[part]) + size_of(hbm["rope_cache"].at[part])
        landed(total, cache_sem.at[g])

    groups = rows // GROUP
    def begin(g):
        if g < groups:
            for copy in cache_copies(g):
                copy.start()

    load(first)
    for name in small:
        load(name).start()
    barrier = pltpu.get_barrier_semaphore()

    @pl.loop(1, devices)
    def _(i):
        pl.semaphore_signal(
            barrier, inc=1, device_id=ident(lax.rem(me + i, devices)), device_id_type=MESH
        )

    load(second)
    begin(0)
    for name in small:
        load(name).wait()
    finish(first)
    begin(1)
    lens = vmem["lengths"]
    ids = vmem["expert_ids"][...]
    slot = iota((slots, rows), 0)
    step = lax.div(slot, block)
    owner = lax.div(step, crew) * crew + lax.rem(lax.rem(step, crew) + seat, crew)
    slot_expert = owner * own_experts + lax.div(lax.rem(slot, block), CAP)
    named = jnp.zeros((slots, rows), F32)
    for k in range(ids.shape[0]):
        named = jnp.where(slot_expert == ids[k : k + 1, :], 1.0, named)
    before = onehot(iota((rows, rows), 0) < iota((rows, rows), 1))
    rank = nn(named.astype(BF16), before)
    taken = jnp.logical_and(named > 0.5, rank == (slot & (CAP - 1)).astype(F32))
    spread_ref[...] = onehot(taken)

    row_id = iota((rows, 128), 0)
    position = jnp.zeros((rows, 128), F32)
    for s in range(rows):
        position = jnp.where(row_id == s, lens[s].astype(F32), position)
    lane = iota((rows, 128), 1)
    half = ROPE // 2
    frequency = jnp.exp((lane & (half - 1)).astype(F32) * (-9.210340371976184 / half))
    angle = position * frequency
    cosine = jnp.cos(angle)
    sine = jnp.sin(angle)
    sine = jnp.where((lane & (ROPE - 1)) < half, -sine, sine)

    tokens = vmem["tokens"][...].astype(F32)
    normed = rms(tokens, vmem["g_attn"][...]).astype(BF16)
    query_low = rms(nn(normed, vmem["w_query_down"][...]), vmem["g_query"][...]).astype(BF16)
    begin(2)
    finish(second)
    query = nn(query_low, vmem["w_query"][...])
    turn = nn(query_low, vmem["w_query_rope"][...])
    rope_width = turn.shape[1]
    rope_lane = iota((rows, rope_width), 1)
    swapped = jnp.where(
        (rope_lane & (ROPE - 1)) < half,
        pltpu.roll(turn, rope_width - half, 1),
        pltpu.roll(turn, half, 1),
    )
    tiles = rope_width // 128
    turned = (
        turn * jnp.concatenate([cosine] * tiles, axis=1)
        + swapped * jnp.concatenate([sine] * tiles, axis=1)
    )
    for h in range(HEADS):
        tile, place = divmod(h * ROPE, 128)
        lanes = turned[:, tile * 128 : (tile + 1) * 128]
        if place:
            lanes = pltpu.roll(lanes, 128 - place, 1)
        qr_ref[h * rows : (h + 1) * rows, :] = lanes
    def put_wide(ref, part, value):
        for t in range(ref.shape[0]):
            ref[t, part, :] = value[:, t * 128 : (t + 1) * 128]

    def get_wide(ref, part):
        return jnp.concatenate([ref[t, part, :] for t in range(ref.shape[0])], axis=1)

    span = 256
    quad = span // NOPE
    quad_lane = iota((rows, span), 1) // NOPE
    w_key_up = vmem["w_key_up"]
    for g in range(3, groups):
        begin(g)
    cache_wait(0)

    def turn_keys(s):
        turned_ref[s % (2 * GROUP)] = vmem["latent_cache"][s].T

    load(third)
    for s in range(GROUP):
        turn_keys(s)
    for n in range(HEADS // quad):
        piece = query[:, n * span : (n + 1) * span]
        spread_query = jnp.concatenate(
            [jnp.where(quad_lane == j, piece, 0.0) for j in range(quad)], axis=0
        )
        put_wide(
            ql_ref,
            pl.ds(n * quad * rows, quad * rows),
            nt(spread_query.astype(BF16), w_key_up[:, n * span : (n + 1) * span]),
        )

    swaps = []
    for p in range(1, tp_size):
        peer = lax.rem(tp + p, tp_size)
        for i, name in enumerate(expert_names):
            swaps.append(
                pltpu.make_async_remote_copy(
                    src_ref=hbm[name].at[pl.ds(peer * own_experts, own_experts)],
                    dst_ref=shard(name, tp),
                    send_sem=swap_send.at[i, p - 1],
                    recv_sem=swap_recv.at[i, p - 1],
                    device_id={"tp": peer},
                    device_id_type=MESH,
                )
            )

    scale = (NOPE + ROPE) ** (-0.5)
    time_lane = iota((HEADS, length), 1)

    def head_rows(s):
        return pl.ds(s, HEADS, stride=rows)

    def score(s):
        query_latent = get_wide(ql_ref, head_rows(s)).astype(BF16)
        query_rope = qr_ref[head_rows(s), :][:, 0:ROPE].astype(BF16)
        found = nn(query_latent, turned_ref[s % (2 * GROUP)])
        return found + nn(query_rope, vmem["rope_cache"][s])

    def soften(s, scores):
        live = time_lane < lens[s]
        scores = jnp.where(live, scores * scale, masked_score)
        top = jnp.max(scores, axis=1, keepdims=True)
        weights = jnp.where(live, jnp.exp(scores - top), 0.0)
        return weights.astype(BF16), jnp.sum(weights, axis=1, keepdims=True)

    def mix(s, weights, total):
        mixed = nn(weights, vmem["latent_cache"][s])
        put_wide(mix_ref, head_rows(s), mixed / total)

    members = [range(g * GROUP, (g + 1) * GROUP) for g in range(groups)]
    scored = []
    for g in range(groups + 1):
        if g + 1 < groups:
            cache_wait(g + 1)
        if g == 0:
            load(fourth)
            load(expert_names)
        if g == max(groups - 2, 0):
            pl.semaphore_wait(barrier, devices - 1)
            for copy in swaps:
                copy.start()
        if g == max(groups - 1, 0):
            finish(third)
        soft = []
        if g > 0:
            soft = [soften(s, scores) for s, scores in zip(members[g - 1], scored)]
        if g < groups:
            scored = [score(s) for s in members[g]]
        if g + 1 < groups:
            for s in members[g + 1]:
                turn_keys(s)
        for s, (weights, total) in zip(members[g - 1], soft):
            mix(s, weights, total)
    value_pieces = []
    for n in range(HEADS // quad):
        part = get_wide(mix_ref, pl.ds(n * quad * rows, quad * rows)).astype(BF16)
        part = nn(part, vmem["w_value_up"][:, n * span : (n + 1) * span])
        piece = part[0:rows]
        for j in range(1, quad):
            piece = jnp.where(quad_lane == j, part[j * rows : (j + 1) * rows], piece)
        value_pieces.append(piece.astype(BF16))
    value_heads = jnp.concatenate(value_pieces, axis=1)
    hidden = (tokens + nn(value_heads, vmem["w_out"][...])).astype(BF16).astype(F32)
    normed_ffn = rms(hidden, vmem["g_ffn"][...]).astype(BF16)
    box = nn(spread_ref[...], normed_ffn).astype(BF16)
    for s in range(devices):
        outbox[s] = box[s * block : (s + 1) * block, :]
    inbox[plane * crew] = outbox[plane * crew]

    def message(src, dst, way, recv, p, i, d):
        return pltpu.make_async_remote_copy(
            src_ref=src.at[p * crew + i],
            dst_ref=dst.at[plane * crew + i],
            send_sem=send_sem.at[way],
            recv_sem=recv,
            device_id=ident(p * crew + d),
            device_id_type=MESH,
        )

    def gate_of(p, i):
        return out_recv.at[2 * p] if isinstance(i, int) and i == 0 else out_recv.at[2 * p + 1]

    def there(p, i):
        d = lax.rem(seat + i, crew)
        return message(outbox, inbox, 0, gate_of(plane, i), p, i, d)

    def back(p, i):
        d = lax.rem(seat + crew - i, crew)
        return message(ret_out, ret_in, 1, back_recv.at[0], p, i, d)

    def bulk(ref, low, size, send, recv):
        part = ref.at[pl.ds(low, size)]
        return pltpu.make_async_remote_copy(
            src_ref=part,
            dst_ref=part,
            send_sem=send,
            recv_sem=recv,
            device_id=ident(me),
            device_id_type=MESH,
        )

    def peers(visit):
        for k in range(planes - 1, -1, -1):
            p = across(k)
            if k:
                visit(p, 0)
            each(1, crew, lambda i, p=p: visit(p, i))
    peers(lambda p, i: there(p, i).start())
    finish(fourth)
    shared_gate = nn(normed_ffn, vmem["w_shared_gate"][...])
    shared_up = nn(normed_ffn, vmem["w_shared_up"][...])
    shared_hidden = (silu(shared_gate) * shared_up).astype(BF16)
    base = hidden + nn(shared_hidden, vmem["w_shared_down"][...])
    latent_new = rms(nn(normed, vmem["w_latent_down"][...]), vmem["g_latent"][...])
    key = nt(normed, vmem["w_rope_key"][...])
    swapped = jnp.concatenate([key[:, half:], key[:, :half]], axis=1)
    key_new = key * cosine[:, :ROPE] + swapped * sine[:, :ROPE]
    kvl = latent_new.shape[1]
    entry_ref[:, 0:kvl] = latent_new.astype(BF16)
    entry_ref[:, kvl : kvl + ROPE] = key_new.astype(BF16)
    route = vmem["route_weights"][...]
    slot_weight = jnp.zeros((slots, rows), F32)
    for k in range(ids.shape[0]):
        hit = slot_expert == ids[k : k + 1, :]
        slot_weight = jnp.where(hit, route[k : k + 1, :], slot_weight)
    slot_weight = jnp.where(spread_ref[...].astype(F32) > 0.5, slot_weight, 0.0)
    high = slot_weight.astype(BF16)
    low = (slot_weight - high.astype(F32)).astype(BF16)
    eye = onehot(iota((rows, rows), 0) == iota((rows, rows), 1))
    weight_high = nt(eye, high).astype(BF16)
    weight_low = nt(eye, low).astype(BF16)
    finish(expert_names)
    for copy in swaps:
        copy.wait()
    gates, ups, downs = (vmem[name] for name in expert_names)

    def serve(p):
        steps = range(p * crew, (p + 1) * crew)
        for e in range(own_experts):
            x = jnp.concatenate(
                [inbox[s, e * CAP : (e + 1) * CAP, :] for s in steps], axis=0
            )
            unit = (silu(nn(x, gates[e])) * nn(x, ups[e])).astype(BF16)
            total = nn(unit, downs[e]).astype(BF16)
            for i, s in enumerate(steps):
                ret_out[s, e * CAP : (e + 1) * CAP, :] = total[i * CAP : (i + 1) * CAP, :]

    for p in range(planes):
        if crew > 1:
            gate = out_recv.at[2 * p + 1]
            bulk(inbox, p * crew + 1, crew - 1, send_sem.at[0], gate).wait_recv()

        @pl.when(plane != p)
        def _():
            bulk(inbox, p * crew, 1, send_sem.at[0], out_recv.at[2 * p]).wait_recv()
        serve(p)
        each(1, crew, lambda i: back(p, i).start())

        @pl.when(plane != p)
        def _():
            back(p, 0).start()

    ret_in[plane * crew] = ret_out[plane * crew]
    remote = devices - 1
    bulk(ret_in, 0, remote, send_sem.at[1], back_recv.at[0]).wait_recv()
    returned = jnp.concatenate([ret_in[s] for s in range(devices)], axis=0)
    both = nn(weight_high, returned) + nn(weight_low, returned)
    out_ref[...] = (base + both).astype(BF16)
    bulk(outbox, 0, remote, send_sem.at[0], back_recv.at[0]).wait_send()
    bulk(ret_out, 0, remote, send_sem.at[1], back_recv.at[0]).wait_send()


def store_kernel(mixed_ref, entry_ref, out_ref, new_ref, sem):
    copies = (
        pltpu.make_async_copy(mixed_ref, out_ref, sem.at[0]),
        pltpu.make_async_copy(entry_ref, new_ref, sem.at[1]),
    )
    for copy in copies:
        copy.start()
    for copy in copies:
        copy.wait()


NAMES = (
    "tokens", "latent_cache", "rope_cache", "expert_ids", "route_weights", "g_attn",
    "w_query_down", "g_query", "w_latent_down", "g_latent", "w_rope_key", "w_query",
    "w_query_rope", "w_key_up", "w_value_up", "w_out", "g_ffn", "w_expert_gate",
    "w_expert_up", "w_expert_down", "w_shared_gate", "w_shared_up", "w_shared_down",
    "lengths",
)


def local(tokens, latent_cache, rope_cache, lengths, expert_ids, route_weights, *weights):
    named = dict(
        zip(NAMES, (tokens, latent_cache, rope_cache, expert_ids, route_weights) + weights + (lengths,))
    )
    for name in ("g_attn", "g_query", "g_latent", "g_ffn"):
        named[name] = named[name].reshape(1, -1)
    named["rope_cache"] = jnp.swapaxes(rope_cache, 1, 2)
    for name in ("expert_ids", "route_weights", "w_rope_key"):
        named[name] = named[name].T
    ep_size = lax.axis_size("ep")
    tp_size = lax.axis_size("tp")
    devices = ep_size * tp_size
    own = named["w_expert_gate"].shape[0] // tp_size
    rows, width = tokens.shape
    pairs = rows * HEADS
    length, kvl = latent_cache.shape[1:]
    slots = devices * own * CAP

    def holder(name):
        shape = named[name].shape
        if name.startswith("w_expert"):
            axis = 1 if name == "w_expert_down" else 2
            shape = (own,) + tuple(
                n * tp_size if i == axis else n for i, n in enumerate(shape) if i
            )
        if name == "lengths":
            return pltpu.SMEM(shape, named[name].dtype)
        return pltpu.VMEM(shape, named[name].dtype)

    box = pltpu.VMEM((devices, own * CAP, width), BF16)
    dma = pltpu.SemaphoreType.DMA
    mixed, entry = pl.pallas_call(
        functools.partial(step_kernel, ep_size, tp_size, NAMES),
        out_shape=(
            pltpu.VMEM((rows, width), BF16),
            pltpu.VMEM((rows, kvl + ROPE), BF16),
        ),
        in_specs=[pl.BlockSpec(memory_space=pl.ANY)] * len(NAMES),
        out_specs=(pl.BlockSpec(memory_space=pltpu.VMEM),) * 2,
        scratch_shapes=[holder(name) for name in NAMES]
        + [
            pltpu.VMEM((kvl // 128, pairs, 128), F32),
            pltpu.VMEM((pairs, 128), F32),
            pltpu.VMEM((kvl // 128, pairs, 128), F32),
            pltpu.VMEM((2 * GROUP, kvl, length), BF16),
            pltpu.VMEM((slots, rows), BF16),
            box,
            box,
            box,
            box,
            dma((7,)),
            dma((5,)),
            dma((rows // GROUP,)),
            dma((3, max(tp_size - 1, 1))),
            dma((3, max(tp_size - 1, 1))),
            dma((2,)),
            dma((2 * (4 if devices % 4 == 0 else 1),)),
            dma((1,)),
        ],
        compiler_params=pltpu.CompilerParams(
            collective_id=0, has_side_effects=True, vmem_limit_bytes=60 * 1024 * 1024
        ),
        name="decode_step",
    )(*[named[name] for name in NAMES])
    return pl.pallas_call(
        store_kernel,
        out_shape=(
            jax.ShapeDtypeStruct(mixed.shape, BF16),
            jax.ShapeDtypeStruct(entry.shape, BF16),
        ),
        in_specs=[pl.BlockSpec(memory_space=pltpu.VMEM)] * 2,
        out_specs=(pl.BlockSpec(memory_space=pl.ANY),) * 2,
        scratch_shapes=[dma((2,))],
        name="store_step",
    )(
        pltpu.with_memory_space_constraint(mixed, pltpu.VMEM),
        pltpu.with_memory_space_constraint(entry, pltpu.VMEM),
    )


def solution(mesh):
    split = ("grp", "ep", "tp")
    in_specs = (
        (P(split, None), P(split, None, None), P(split, None, None), P(split))
        + (P(split, None), P(split, None))
        + (P(),) * 12
        + (P("ep", None, "tp"), P("ep", None, "tp"), P("ep", "tp", None))
        + (P(),) * 3
    )
    out_specs = (P(split, None), P(split, None))
    return jax.shard_map(local, mesh=mesh, in_specs=in_specs, out_specs=out_specs, check_vma=False)
```

```python
import functools
import math

import jax
import jax.numpy as jnp
from jax import lax
from jax.experimental import pallas as pl
from jax.experimental.pallas import tpu as pltpu
from jax.sharding import PartitionSpec as P

HEADS = 16
NOPE = 64
ROPE = 32
VDIM = 64
CAP = 4

norm_eps = 1e-06
masked_score = -1e30
F32 = jnp.float32
BF16 = jnp.bfloat16
MESH = pl.DeviceIdType.MESH


def nn(a, b):
    return jnp.dot(a, b, preferred_element_type=F32)


def nt(a, b):
    return lax.dot_general(a, b, (((1,), (1,)), ((), ())), preferred_element_type=F32)


def iota(shape, axis):
    return lax.broadcasted_iota(jnp.int32, shape, axis)


def rms(values, gain):
    mean_square = jnp.mean(values * values, axis=-1, keepdims=True)
    return values * lax.rsqrt(mean_square + norm_eps) * gain


def silu(v):
    return v / (1.0 + jnp.exp(-v))


def onehot(cond):
    return jnp.where(cond, 1.0, 0.0).astype(BF16)


def group_sizes(rows):
    return [rows // 4, 3 * rows // 8, rows - rows // 4 - 3 * rows // 8]


def step_kernel(ep_size, tp_size, names, *refs):
    count = len(names)
    hbm = dict(zip(names, refs[:count]))
    out_ref, entry_ref = refs[count : count + 2]
    refs = refs[count + 2 :]
    vmem = dict(zip(names, refs[:count]))
    (
        ql_ref,
        qr_ref,
        mix_ref,
        turned_ref,
        spread_ref,
        outbox,
        inbox,
        ret_out,
        ret_in,
        small_sem,
        load_sem,
        cache_sem,
        swap_send,
        swap_recv,
        send_sem,
        out_recv,
        back_recv,
    ) = refs[count:]
    rows, width = hbm["tokens"].shape
    length = hbm["latent_cache"].shape[1]
    own_experts = vmem["w_expert_gate"].shape[0]
    devices = ep_size * tp_size
    block = own_experts * CAP
    slots = devices * block
    ep = lax.axis_index("ep")
    tp = lax.axis_index("tp")
    me = ep * tp_size + tp
    planes = 4 if devices % 4 == 0 else 1
    crew = devices // planes
    plane = me // crew
    seat = me % crew

    def across(k):
        total = 0
        for b in range(planes.bit_length() - 1):
            total = total + ((plane // (1 << b) + (k >> b)) % 2) * (1 << b)
        return total

    def ident(d):
        return {"ep": d // tp_size, "tp": d % tp_size}

    def each(low, high, visit):
        if high - low <= 16:
            for i in range(low, high):
                visit(i)
        else:
            pl.loop(low, high)(visit)

    expert_names = ("w_expert_gate", "w_expert_up", "w_expert_down")

    def shard(name, owner):
        axis = 1 if name == "w_expert_down" else 2
        units = hbm[name].shape[axis]
        part = pl.ds(pl.multiple_of(owner * units, units), units)
        if axis == 1:
            return vmem[name].at[:, part, :]
        return vmem[name].at[:, :, part]

    small = (
        "lengths", "expert_ids", "route_weights", "g_attn", "g_query", "g_latent", "g_ffn",
    )
    first = ("tokens", "w_query_down")
    second = ("w_query", "w_query_rope", "w_key_up")
    third = ("w_value_up", "w_out")
    fourth = (
        "w_shared_gate", "w_shared_up", "w_shared_down", "w_latent_down", "w_rope_key",
    )
    batches = (first, second, third, fourth, expert_names)

    def source_of(name):
        if name in expert_names:
            return hbm[name].at[pl.ds(tp * own_experts, own_experts)]
        return hbm[name]

    def load(batch):
        if batch in small:
            sem = small_sem.at[small.index(batch)]
            return pltpu.make_async_copy(hbm[batch], vmem[batch], sem)
        sem = load_sem.at[batches.index(batch)]
        for name in batch:
            place = shard(name, tp) if name in expert_names else vmem[name]
            pltpu.make_async_copy(source_of(name), place, sem).start()

    def size_of(ref):
        return math.prod(ref.shape) * jnp.dtype(ref.dtype).itemsize

    def landed(total, sem):
        cache = hbm["latent_cache"]
        row = cache.shape[2] * 2
        shapes = [
            (n, total // (n * row))
            for n in range(1, rows + 1)
            if total % (16 * n * row) == 0 and total // (n * row) <= length
        ]
        n, depth = shapes[0]
        part = (pl.ds(0, n), pl.ds(0, depth))
        pltpu.make_async_copy(cache.at[part], vmem["latent_cache"].at[part], sem).wait()

    def finish(batch):
        total = sum(size_of(source_of(name)) for name in batch)
        landed(total, load_sem.at[batches.index(batch)])

    def cache_copies(g):
        part = pl.ds(members[g][0], len(members[g]))
        return (
            pltpu.make_async_copy(
                hbm["latent_cache"].at[part], vmem["latent_cache"].at[part], cache_sem.at[g]
            ),
            pltpu.make_async_copy(
                hbm["rope_cache"].at[part], vmem["rope_cache"].at[part], cache_sem.at[g]
            ),
        )

    def cache_wait(g):
        part = pl.ds(0, len(members[g]))
        total = size_of(hbm["latent_cache"].at[part]) + size_of(hbm["rope_cache"].at[part])
        landed(total, cache_sem.at[g])

    sizes = group_sizes(rows)
    groups = len(sizes)
    members = [range(sum(sizes[:g]), sum(sizes[: g + 1])) for g in range(groups)]

    def begin(g):
        if g < groups:
            for copy in cache_copies(g):
                copy.start()

    load(first)
    for name in small:
        load(name).start()
    barrier = pltpu.get_barrier_semaphore()

    @pl.loop(1, devices)
    def _(i):
        pl.semaphore_signal(
            barrier, inc=1, device_id=ident(lax.rem(me + i, devices)), device_id_type=MESH
        )

    load(second)
    begin(0)
    for name in small:
        load(name).wait()
    finish(first)
    begin(1)
    lens = vmem["lengths"]
    ids = vmem["expert_ids"][...]
    slot = iota((slots, rows), 0)
    step = lax.div(slot, block)
    owner = lax.div(step, crew) * crew + lax.rem(lax.rem(step, crew) + seat, crew)
    slot_expert = owner * own_experts + lax.div(lax.rem(slot, block), CAP)
    named = jnp.zeros((slots, rows), F32)
    for k in range(ids.shape[0]):
        named = jnp.where(slot_expert == ids[k : k + 1, :], 1.0, named)
    before = onehot(iota((rows, rows), 0) < iota((rows, rows), 1))
    rank = nn(named.astype(BF16), before)
    taken = jnp.logical_and(named > 0.5, rank == (slot & (CAP - 1)).astype(F32))
    spread_ref[...] = onehot(taken)

    row_id = iota((rows, 128), 0)
    position = jnp.zeros((rows, 128), F32)
    for s in range(rows):
        position = jnp.where(row_id == s, lens[s].astype(F32), position)
    lane = iota((rows, 128), 1)
    half = ROPE // 2
    frequency = jnp.exp((lane & (half - 1)).astype(F32) * (-9.210340371976184 / half))
    angle = position * frequency
    cosine = jnp.cos(angle)
    sine = jnp.sin(angle)
    sine = jnp.where((lane & (ROPE - 1)) < half, -sine, sine)

    tokens = vmem["tokens"][...].astype(F32)
    normed = rms(tokens, vmem["g_attn"][...]).astype(BF16)
    query_low = rms(nn(normed, vmem["w_query_down"][...]), vmem["g_query"][...]).astype(BF16)
    finish(second)
    begin(2)
    query = nn(query_low, vmem["w_query"][...])
    turn = nn(query_low, vmem["w_query_rope"][...])
    rope_width = turn.shape[1]
    rope_lane = iota((rows, rope_width), 1)
    swapped = jnp.where(
        (rope_lane & (ROPE - 1)) < half,
        pltpu.roll(turn, rope_width - half, 1),
        pltpu.roll(turn, half, 1),
    )
    tiles = rope_width // 128
    turned = (
        turn * jnp.concatenate([cosine] * tiles, axis=1)
        + swapped * jnp.concatenate([sine] * tiles, axis=1)
    )
    for h in range(HEADS):
        tile, place = divmod(h * ROPE, 128)
        lanes = turned[:, tile * 128 : (tile + 1) * 128]
        if place:
            lanes = pltpu.roll(lanes, 128 - place, 1)
        qr_ref[h * rows : (h + 1) * rows, :] = lanes
    def put_wide(ref, part, value):
        for t in range(ref.shape[0]):
            ref[t, part, :] = value[:, t * 128 : (t + 1) * 128]

    def get_wide(ref, part):
        return jnp.concatenate([ref[t, part, :] for t in range(ref.shape[0])], axis=1)

    span = 256
    quad = span // NOPE
    quad_lane = iota((rows, span), 1) // NOPE
    w_key_up = vmem["w_key_up"]

    cut = 3 * length // 4

    def turn_keys(s):
        turned_ref[s] = vmem["latent_cache"][s, 0:cut, :].T

    for n in range(HEADS // quad):
        piece = query[:, n * span : (n + 1) * span]
        spread_query = jnp.concatenate(
            [jnp.where(quad_lane == j, piece, 0.0) for j in range(quad)], axis=0
        )
        put_wide(
            ql_ref,
            pl.ds(n * quad * rows, quad * rows),
            nt(spread_query.astype(BF16), w_key_up[:, n * span : (n + 1) * span]),
        )

    swaps = []
    for p in range(1, tp_size):
        peer = lax.rem(tp + p, tp_size)
        for i, name in enumerate(expert_names):
            swaps.append(
                pltpu.make_async_remote_copy(
                    src_ref=hbm[name].at[pl.ds(peer * own_experts, own_experts)],
                    dst_ref=shard(name, tp),
                    send_sem=swap_send.at[i, p - 1],
                    recv_sem=swap_recv.at[i, p - 1],
                    device_id={"tp": peer},
                    device_id_type=MESH,
                )
            )

    scale = (NOPE + ROPE) ** (-0.5)
    time_lane = iota((HEADS, length), 1)

    def head_rows(s):
        return pl.ds(s, HEADS, stride=rows)

    def score(s):
        query_latent = get_wide(ql_ref, head_rows(s)).astype(BF16)
        query_rope = qr_ref[head_rows(s), :][:, 0:ROPE].astype(BF16)
        found = nn(query_latent, turned_ref[s])
        if cut < length:
            rest = nt(query_latent, vmem["latent_cache"][s, cut:length, :])
            found = jnp.concatenate([found, rest], axis=1)
        return found + nn(query_rope, vmem["rope_cache"][s])

    def soften(s, scores):
        live = time_lane < lens[s]
        scores = jnp.where(live, scores * scale, masked_score)
        top = jnp.max(scores, axis=1, keepdims=True)
        weights = jnp.where(live, jnp.exp(scores - top), 0.0)
        return weights.astype(BF16), jnp.sum(weights, axis=1, keepdims=True)

    def mix(s, weights, total):
        mixed = nn(weights, vmem["latent_cache"][s])
        put_wide(mix_ref, head_rows(s), mixed / total)

    for g in range(groups):
        cache_wait(g)
        if g == 0:
            for later in range(3, groups):
                begin(later)
        if g == 0:
            load(third)
        if g == groups - 1:
            load(fourth)
            load(expert_names)
        for s in members[g]:
            turn_keys(s)
        scored = [score(s) for s in members[g]]
        soft = [soften(s, scores) for s, scores in zip(members[g], scored)]
        for s, (weights, total) in zip(members[g], soft):
            mix(s, weights, total)
    finish(third)
    pl.semaphore_wait(barrier, devices - 1)
    for copy in swaps:
        copy.start()
    value_pieces = []
    for n in range(HEADS // quad):
        part = get_wide(mix_ref, pl.ds(n * quad * rows, quad * rows)).astype(BF16)
        part = nn(part, vmem["w_value_up"][:, n * span : (n + 1) * span])
        piece = part[0:rows]
        for j in range(1, quad):
            piece = jnp.where(quad_lane == j, part[j * rows : (j + 1) * rows], piece)
        value_pieces.append(piece.astype(BF16))
    value_heads = jnp.concatenate(value_pieces, axis=1)
    hidden = (tokens + nn(value_heads, vmem["w_out"][...])).astype(BF16).astype(F32)
    normed_ffn = rms(hidden, vmem["g_ffn"][...]).astype(BF16)
    box = nn(spread_ref[...], normed_ffn).astype(BF16)
    for s in range(devices):
        outbox[s] = box[s * block : (s + 1) * block, :]
    inbox[plane * crew] = outbox[plane * crew]

    def message(src, dst, way, recv, p, i, d):
        return pltpu.make_async_remote_copy(
            src_ref=src.at[p * crew + i],
            dst_ref=dst.at[plane * crew + i],
            send_sem=send_sem.at[way],
            recv_sem=recv,
            device_id=ident(p * crew + d),
            device_id_type=MESH,
        )

    def gate_of(p, i):
        return out_recv.at[2 * p] if isinstance(i, int) and i == 0 else out_recv.at[2 * p + 1]

    def there(p, i):
        d = lax.rem(seat + i, crew)
        return message(outbox, inbox, 0, gate_of(plane, i), p, i, d)

    def back(p, i):
        d = lax.rem(seat + crew - i, crew)
        return message(ret_out, ret_in, 1, back_recv.at[0], p, i, d)

    def bulk(ref, low, size, send, recv):
        part = ref.at[pl.ds(low, size)]
        return pltpu.make_async_remote_copy(
            src_ref=part,
            dst_ref=part,
            send_sem=send,
            recv_sem=recv,
            device_id=ident(me),
            device_id_type=MESH,
        )

    def peers(visit):
        for k in range(planes - 1, -1, -1):
            p = across(k)
            if k:
                visit(p, 0)
            each(1, crew, lambda i, p=p: visit(p, i))
    peers(lambda p, i: there(p, i).start())
    finish(fourth)
    shared_gate = nn(normed_ffn, vmem["w_shared_gate"][...])
    shared_up = nn(normed_ffn, vmem["w_shared_up"][...])
    shared_hidden = (silu(shared_gate) * shared_up).astype(BF16)
    base = hidden + nn(shared_hidden, vmem["w_shared_down"][...])
    latent_new = rms(nn(normed, vmem["w_latent_down"][...]), vmem["g_latent"][...])
    key = nt(normed, vmem["w_rope_key"][...])
    swapped = jnp.concatenate([key[:, half:], key[:, :half]], axis=1)
    key_new = key * cosine[:, :ROPE] + swapped * sine[:, :ROPE]
    kvl = latent_new.shape[1]
    entry_ref[:, 0:kvl] = latent_new.astype(BF16)
    entry_ref[:, kvl : kvl + ROPE] = key_new.astype(BF16)
    route = vmem["route_weights"][...]
    slot_weight = jnp.zeros((slots, rows), F32)
    for k in range(ids.shape[0]):
        hit = slot_expert == ids[k : k + 1, :]
        slot_weight = jnp.where(hit, route[k : k + 1, :], slot_weight)
    slot_weight = jnp.where(spread_ref[...].astype(F32) > 0.5, slot_weight, 0.0)
    high = slot_weight.astype(BF16)
    low = (slot_weight - high.astype(F32)).astype(BF16)
    eye = onehot(iota((rows, rows), 0) == iota((rows, rows), 1))
    weight_high = nt(eye, high).astype(BF16)
    weight_low = nt(eye, low).astype(BF16)
    finish(expert_names)
    for copy in swaps:
        copy.wait()
    gates, ups, downs = (vmem[name] for name in expert_names)

    def serve(low, high):
        steps = range(low * crew, high * crew)
        for e in range(own_experts):
            x = jnp.concatenate(
                [inbox[s, e * CAP : (e + 1) * CAP, :] for s in steps], axis=0
            )
            unit = (silu(nn(x, gates[e])) * nn(x, ups[e])).astype(BF16)
            total = nn(unit, downs[e]).astype(BF16)
            for i, s in enumerate(steps):
                ret_out[s, e * CAP : (e + 1) * CAP, :] = total[i * CAP : (i + 1) * CAP, :]

    def collect(p):
        if crew > 1:
            gate = out_recv.at[2 * p + 1]
            bulk(inbox, p * crew + 1, crew - 1, send_sem.at[0], gate).wait_recv()

        @pl.when(plane != p)
        def _():
            bulk(inbox, p * crew, 1, send_sem.at[0], out_recv.at[2 * p]).wait_recv()

    def give(p):
        @pl.when(plane != p)
        def _():
            back(p, 0).start()

        each(1, crew, lambda i: back(p, i).start())

    chunks = ((0, 1), (1, 2), (2, 3), (3, 4))
    for low, high in chunks if planes == 4 else [(0, planes)]:
        for p in range(low, high):
            collect(p)
        serve(low, high)
        for p in range(low, high):
            give(p)

    ret_in[plane * crew] = ret_out[plane * crew]
    remote = devices - 1
    bulk(ret_in, 0, remote, send_sem.at[1], back_recv.at[0]).wait_recv()
    returned = jnp.concatenate([ret_in[s] for s in range(devices)], axis=0)
    both = nn(weight_high, returned) + nn(weight_low, returned)
    out_ref[...] = (base + both).astype(BF16)
    bulk(outbox, 0, remote, send_sem.at[0], back_recv.at[0]).wait_send()
    bulk(ret_out, 0, remote, send_sem.at[1], back_recv.at[0]).wait_send()


def store_kernel(mixed_ref, entry_ref, out_ref, new_ref, sem):
    copies = (
        pltpu.make_async_copy(mixed_ref, out_ref, sem.at[0]),
        pltpu.make_async_copy(entry_ref, new_ref, sem.at[1]),
    )
    for copy in copies:
        copy.start()
    for copy in copies:
        copy.wait()


NAMES = (
    "tokens", "latent_cache", "rope_cache", "expert_ids", "route_weights", "g_attn",
    "w_query_down", "g_query", "w_latent_down", "g_latent", "w_rope_key", "w_query",
    "w_query_rope", "w_key_up", "w_value_up", "w_out", "g_ffn", "w_expert_gate",
    "w_expert_up", "w_expert_down", "w_shared_gate", "w_shared_up", "w_shared_down",
    "lengths",
)


def local(tokens, latent_cache, rope_cache, lengths, expert_ids, route_weights, *weights):
    named = dict(
        zip(NAMES, (tokens, latent_cache, rope_cache, expert_ids, route_weights) + weights + (lengths,))
    )
    for name in ("g_attn", "g_query", "g_latent", "g_ffn"):
        named[name] = named[name].reshape(1, -1)
    named["rope_cache"] = jnp.swapaxes(rope_cache, 1, 2)
    for name in ("expert_ids", "route_weights", "w_rope_key"):
        named[name] = named[name].T
    ep_size = lax.axis_size("ep")
    tp_size = lax.axis_size("tp")
    devices = ep_size * tp_size
    own = named["w_expert_gate"].shape[0] // tp_size
    rows, width = tokens.shape
    pairs = rows * HEADS
    length, kvl = latent_cache.shape[1:]
    slots = devices * own * CAP

    def holder(name):
        shape = named[name].shape
        if name.startswith("w_expert"):
            axis = 1 if name == "w_expert_down" else 2
            shape = (own,) + tuple(
                n * tp_size if i == axis else n for i, n in enumerate(shape) if i
            )
        if name == "lengths":
            return pltpu.SMEM(shape, named[name].dtype)
        return pltpu.VMEM(shape, named[name].dtype)

    box = pltpu.VMEM((devices, own * CAP, width), BF16)
    dma = pltpu.SemaphoreType.DMA
    mixed, entry = pl.pallas_call(
        functools.partial(step_kernel, ep_size, tp_size, NAMES),
        out_shape=(
            pltpu.VMEM((rows, width), BF16),
            pltpu.VMEM((rows, kvl + ROPE), BF16),
        ),
        in_specs=[pl.BlockSpec(memory_space=pl.ANY)] * len(NAMES),
        out_specs=(pl.BlockSpec(memory_space=pltpu.VMEM),) * 2,
        scratch_shapes=[holder(name) for name in NAMES]
        + [
            pltpu.VMEM((kvl // 128, pairs, 128), F32),
            pltpu.VMEM((pairs, 128), F32),
            pltpu.VMEM((kvl // 128, pairs, 128), F32),
            pltpu.VMEM((rows, kvl, 3 * length // 4), BF16),
            pltpu.VMEM((slots, rows), BF16),
            box,
            box,
            box,
            box,
            dma((7,)),
            dma((5,)),
            dma((len(group_sizes(rows)),)),
            dma((3, max(tp_size - 1, 1))),
            dma((3, max(tp_size - 1, 1))),
            dma((2,)),
            dma((2 * (4 if devices % 4 == 0 else 1),)),
            dma((1,)),
        ],
        compiler_params=pltpu.CompilerParams(
            collective_id=0, has_side_effects=True, vmem_limit_bytes=60 * 1024 * 1024
        ),
        name="decode_step",
    )(*[named[name] for name in NAMES])
    return pl.pallas_call(
        store_kernel,
        out_shape=(
            jax.ShapeDtypeStruct(mixed.shape, BF16),
            jax.ShapeDtypeStruct(entry.shape, BF16),
        ),
        in_specs=[pl.BlockSpec(memory_space=pltpu.VMEM)] * 2,
        out_specs=(pl.BlockSpec(memory_space=pl.ANY),) * 2,
        scratch_shapes=[dma((2,))],
        name="store_step",
    )(
        pltpu.with_memory_space_constraint(mixed, pltpu.VMEM),
        pltpu.with_memory_space_constraint(entry, pltpu.VMEM),
    )


def solution(mesh):
    split = ("grp", "ep", "tp")
    in_specs = (
        (P(split, None), P(split, None, None), P(split, None, None), P(split))
        + (P(split, None), P(split, None))
        + (P(),) * 12
        + (P("ep", None, "tp"), P("ep", None, "tp"), P("ep", "tp", None))
        + (P(),) * 3
    )
    out_specs = (P(split, None), P(split, None))
    return jax.shard_map(local, mesh=mesh, in_specs=in_specs, out_specs=out_specs, check_vma=False)
```

```python
import functools
import math

import jax
import jax.numpy as jnp
from jax import lax
from jax.experimental import pallas as pl
from jax.experimental.pallas import tpu as pltpu
from jax.sharding import PartitionSpec as P

HEADS = 16
NOPE = 64
ROPE = 32
VDIM = 64
CAP = 4

norm_eps = 1e-06
masked_score = -1e30
F32 = jnp.float32
BF16 = jnp.bfloat16
MESH = pl.DeviceIdType.MESH


def nn(a, b):
    return jnp.dot(a, b, preferred_element_type=F32)


def nt(a, b):
    return lax.dot_general(a, b, (((1,), (1,)), ((), ())), preferred_element_type=F32)


def iota(shape, axis):
    return lax.broadcasted_iota(jnp.int32, shape, axis)


def rms(values, gain):
    mean_square = jnp.mean(values * values, axis=-1, keepdims=True)
    return values * lax.rsqrt(mean_square + norm_eps) * gain


def silu(v):
    return v / (1.0 + jnp.exp(-v))


def onehot(cond):
    return jnp.where(cond, 1.0, 0.0).astype(BF16)


def group_sizes(rows):
    return [rows // 4, 3 * rows // 8, rows - rows // 4 - 3 * rows // 8]


def step_kernel(ep_size, tp_size, names, *refs):
    count = len(names)
    hbm = dict(zip(names, refs[:count]))
    out_ref, entry_ref = refs[count : count + 2]
    refs = refs[count + 2 :]
    vmem = dict(zip(names, refs[:count]))
    (
        ql_ref,
        qr_ref,
        mix_ref,
        turned_ref,
        spread_ref,
        outbox,
        inbox,
        ret_out,
        ret_in,
        small_sem,
        load_sem,
        cache_sem,
        swap_send,
        swap_recv,
        send_sem,
        out_recv,
        back_recv,
    ) = refs[count:]
    rows, width = hbm["tokens"].shape
    length = hbm["latent_cache"].shape[1]
    own_experts = vmem["w_expert_gate"].shape[0]
    devices = ep_size * tp_size
    block = own_experts * CAP
    slots = devices * block
    ep = lax.axis_index("ep")
    tp = lax.axis_index("tp")
    me = ep * tp_size + tp
    planes = 4 if devices % 4 == 0 else 1
    crew = devices // planes
    plane = me // crew
    seat = me % crew

    def across(k):
        total = 0
        for b in range(planes.bit_length() - 1):
            total = total + ((plane // (1 << b) + (k >> b)) % 2) * (1 << b)
        return total

    def ident(d):
        return {"ep": d // tp_size, "tp": d % tp_size}

    def each(low, high, visit):
        if high - low <= 16:
            for i in range(low, high):
                visit(i)
        else:
            pl.loop(low, high)(visit)

    expert_names = ("w_expert_gate", "w_expert_up", "w_expert_down")

    def shard(name, owner):
        axis = 1 if name == "w_expert_down" else 2
        units = hbm[name].shape[axis]
        part = pl.ds(pl.multiple_of(owner * units, units), units)
        if axis == 1:
            return vmem[name].at[:, part, :]
        return vmem[name].at[:, :, part]

    small = (
        "g_attn", "g_query", "lengths", "expert_ids", "route_weights", "g_latent", "g_ffn",
    )
    first = ("tokens", "w_query_down")
    second = ("w_query", "w_query_rope", "w_key_up")
    third = ("w_value_up", "w_out")
    fourth = (
        "w_shared_gate", "w_shared_up", "w_shared_down", "w_latent_down", "w_rope_key",
    )
    batches = (first, second, third, fourth, expert_names)

    def source_of(name):
        if name in expert_names:
            return hbm[name].at[pl.ds(tp * own_experts, own_experts)]
        return hbm[name]

    def load(batch):
        if batch in small:
            sem = small_sem.at[small.index(batch)]
            return pltpu.make_async_copy(hbm[batch], vmem[batch], sem)
        sem = load_sem.at[batches.index(batch)]
        for name in batch:
            place = shard(name, tp) if name in expert_names else vmem[name]
            pltpu.make_async_copy(source_of(name), place, sem).start()

    def size_of(ref):
        return math.prod(ref.shape) * jnp.dtype(ref.dtype).itemsize

    def landed(total, sem):
        cache = hbm["latent_cache"]
        row = cache.shape[2] * 2
        shapes = [
            (n, total // (n * row))
            for n in range(1, rows + 1)
            if total % (16 * n * row) == 0 and total // (n * row) <= length
        ]
        n, depth = shapes[0]
        part = (pl.ds(0, n), pl.ds(0, depth))
        pltpu.make_async_copy(cache.at[part], vmem["latent_cache"].at[part], sem).wait()

    def finish(batch):
        total = sum(size_of(source_of(name)) for name in batch)
        landed(total, load_sem.at[batches.index(batch)])

    def cache_copies(g):
        part = pl.ds(members[g][0], len(members[g]))
        return (
            pltpu.make_async_copy(
                hbm["latent_cache"].at[part], vmem["latent_cache"].at[part], cache_sem.at[g]
            ),
            pltpu.make_async_copy(
                hbm["rope_cache"].at[part], vmem["rope_cache"].at[part], cache_sem.at[g]
            ),
        )

    def cache_wait(g):
        part = pl.ds(0, len(members[g]))
        total = size_of(hbm["latent_cache"].at[part]) + size_of(hbm["rope_cache"].at[part])
        landed(total, cache_sem.at[g])

    sizes = group_sizes(rows)
    groups = len(sizes)
    members = [range(sum(sizes[:g]), sum(sizes[: g + 1])) for g in range(groups)]

    def begin(g):
        if g < groups:
            for copy in cache_copies(g):
                copy.start()

    load(first)
    for name in small:
        load(name).start()
    barrier = pltpu.get_barrier_semaphore()

    @pl.loop(1, devices)
    def _(i):
        pl.semaphore_signal(
            barrier, inc=1, device_id=ident(lax.rem(me + i, devices)), device_id_type=MESH
        )

    load(second)
    begin(0)
    load("g_attn").wait()
    load("g_query").wait()
    finish(first)
    begin(1)
    tokens = vmem["tokens"][...].astype(F32)
    normed = rms(tokens, vmem["g_attn"][...]).astype(BF16)
    query_low = rms(nn(normed, vmem["w_query_down"][...]), vmem["g_query"][...]).astype(BF16)
    finish(second)
    begin(2)
    for name in small:
        if name not in ("g_attn", "g_query"):
            load(name).wait()
    lens = vmem["lengths"]
    ids = vmem["expert_ids"][...]
    slot = iota((slots, rows), 0)
    step = lax.div(slot, block)
    owner = lax.div(step, crew) * crew + lax.rem(lax.rem(step, crew) + seat, crew)
    slot_expert = owner * own_experts + lax.div(lax.rem(slot, block), CAP)
    named = jnp.zeros((slots, rows), F32)
    for k in range(ids.shape[0]):
        named = jnp.where(slot_expert == ids[k : k + 1, :], 1.0, named)
    before = onehot(iota((rows, rows), 0) < iota((rows, rows), 1))
    rank = nn(named.astype(BF16), before)
    taken = jnp.logical_and(named > 0.5, rank == (slot & (CAP - 1)).astype(F32))
    spread_ref[...] = onehot(taken)

    row_id = iota((rows, 128), 0)
    position = jnp.zeros((rows, 128), F32)
    for s in range(rows):
        position = jnp.where(row_id == s, lens[s].astype(F32), position)
    lane = iota((rows, 128), 1)
    half = ROPE // 2
    frequency = jnp.exp((lane & (half - 1)).astype(F32) * (-9.210340371976184 / half))
    angle = position * frequency
    cosine = jnp.cos(angle)
    sine = jnp.sin(angle)
    sine = jnp.where((lane & (ROPE - 1)) < half, -sine, sine)

    query = nn(query_low, vmem["w_query"][...])
    turn = nn(query_low, vmem["w_query_rope"][...])
    rope_width = turn.shape[1]
    rope_lane = iota((rows, rope_width), 1)
    swapped = jnp.where(
        (rope_lane & (ROPE - 1)) < half,
        pltpu.roll(turn, rope_width - half, 1),
        pltpu.roll(turn, half, 1),
    )
    tiles = rope_width // 128
    turned = (
        turn * jnp.concatenate([cosine] * tiles, axis=1)
        + swapped * jnp.concatenate([sine] * tiles, axis=1)
    )
    for h in range(HEADS):
        tile, place = divmod(h * ROPE, 128)
        lanes = turned[:, tile * 128 : (tile + 1) * 128]
        if place:
            lanes = pltpu.roll(lanes, 128 - place, 1)
        qr_ref[h * rows : (h + 1) * rows, :] = lanes
    def put_wide(ref, part, value):
        for t in range(ref.shape[0]):
            ref[t, part, :] = value[:, t * 128 : (t + 1) * 128]

    def get_wide(ref, part):
        return jnp.concatenate([ref[t, part, :] for t in range(ref.shape[0])], axis=1)

    span = 256
    quad = span // NOPE
    quad_lane = iota((rows, span), 1) // NOPE
    w_key_up = vmem["w_key_up"]

    quarters = (0, 2, 4, 4, 3, 3)
    cuts = {}
    for group in members:
        for i, s in enumerate(group):
            cuts[s] = quarters[min(i, len(quarters) - 1)] * length // 4

    def turn_keys(s):
        if cuts[s]:
            turned_ref[s, :, 0 : cuts[s]] = vmem["latent_cache"][s, 0 : cuts[s], :].T

    for n in range(HEADS // quad):
        piece = query[:, n * span : (n + 1) * span]
        spread_query = jnp.concatenate(
            [jnp.where(quad_lane == j, piece, 0.0) for j in range(quad)], axis=0
        )
        put_wide(
            ql_ref,
            pl.ds(n * quad * rows, quad * rows),
            nt(spread_query.astype(BF16), w_key_up[:, n * span : (n + 1) * span]),
        )

    swaps = []
    for p in range(1, tp_size):
        peer = lax.rem(tp + p, tp_size)
        for i, name in enumerate(expert_names):
            swaps.append(
                pltpu.make_async_remote_copy(
                    src_ref=hbm[name].at[pl.ds(peer * own_experts, own_experts)],
                    dst_ref=shard(name, tp),
                    send_sem=swap_send.at[i, p - 1],
                    recv_sem=swap_recv.at[i, p - 1],
                    device_id={"tp": peer},
                    device_id_type=MESH,
                )
            )

    scale = (NOPE + ROPE) ** (-0.5)
    time_lane = iota((HEADS, length), 1)

    def head_rows(s):
        return pl.ds(s, HEADS, stride=rows)

    def score(s):
        query_latent = get_wide(ql_ref, head_rows(s)).astype(BF16)
        query_rope = qr_ref[head_rows(s), :][:, 0:ROPE].astype(BF16)
        cut = cuts[s]
        pieces = []
        if cut > 0:
            pieces.append(nn(query_latent, turned_ref[s, :, 0:cut]))
        if cut < length:
            pieces.append(nt(query_latent, vmem["latent_cache"][s, cut:length, :]))
        found = pieces[0] if len(pieces) == 1 else jnp.concatenate(pieces, axis=1)
        return found + nn(query_rope, vmem["rope_cache"][s])

    def soften(s, scores):
        live = time_lane < lens[s]
        scores = jnp.where(live, scores * scale, masked_score)
        top = jnp.max(scores, axis=1, keepdims=True)
        weights = jnp.exp(scores - top)
        return weights.astype(BF16), jnp.sum(weights, axis=1, keepdims=True)

    def mix(s, weights, total):
        mixed = nn(weights, vmem["latent_cache"][s])
        put_wide(mix_ref, head_rows(s), mixed / total)

    for g in range(groups):
        cache_wait(g)
        if g == 0:
            for later in range(3, groups):
                begin(later)
        if g == 0:
            load(third)
        if g == groups - 1:
            load(fourth)
            load(expert_names)
        for s in members[g]:
            turn_keys(s)
        scored = [score(s) for s in members[g]]
        soft = [soften(s, scores) for s, scores in zip(members[g], scored)]
        for s, (weights, total) in zip(members[g], soft):
            mix(s, weights, total)
    finish(third)
    pl.semaphore_wait(barrier, devices - 1)
    for copy in swaps:
        copy.start()
    value_pieces = []
    for n in range(HEADS // quad):
        part = get_wide(mix_ref, pl.ds(n * quad * rows, quad * rows)).astype(BF16)
        part = nn(part, vmem["w_value_up"][:, n * span : (n + 1) * span])
        piece = part[0:rows]
        for j in range(1, quad):
            piece = jnp.where(quad_lane == j, part[j * rows : (j + 1) * rows], piece)
        value_pieces.append(piece.astype(BF16))
    value_heads = jnp.concatenate(value_pieces, axis=1)
    hidden = (tokens + nn(value_heads, vmem["w_out"][...])).astype(BF16).astype(F32)
    normed_ffn = rms(hidden, vmem["g_ffn"][...]).astype(BF16)
    box = nn(spread_ref[...], normed_ffn).astype(BF16)
    for s in range(devices):
        outbox[s] = box[s * block : (s + 1) * block, :]
    inbox[plane * crew] = outbox[plane * crew]

    def message(src, dst, way, recv, p, i, d):
        return pltpu.make_async_remote_copy(
            src_ref=src.at[p * crew + i],
            dst_ref=dst.at[plane * crew + i],
            send_sem=send_sem.at[way],
            recv_sem=recv,
            device_id=ident(p * crew + d),
            device_id_type=MESH,
        )

    def gate_of(p, i):
        return out_recv.at[2 * p] if isinstance(i, int) and i == 0 else out_recv.at[2 * p + 1]

    def there(p, i):
        d = lax.rem(seat + i, crew)
        return message(outbox, inbox, 0, gate_of(plane, i), p, i, d)

    def back(p, i):
        d = lax.rem(seat + crew - i, crew)
        return message(ret_out, ret_in, 1, back_recv.at[0], p, i, d)

    def bulk(ref, low, size, send, recv):
        part = ref.at[pl.ds(low, size)]
        return pltpu.make_async_remote_copy(
            src_ref=part,
            dst_ref=part,
            send_sem=send,
            recv_sem=recv,
            device_id=ident(me),
            device_id_type=MESH,
        )

    def peers(visit):
        for k in range(planes - 1, -1, -1):
            p = across(k)
            if k:
                visit(p, 0)
            each(1, crew, lambda i, p=p: visit(p, i))
    peers(lambda p, i: there(p, i).start())
    finish(fourth)
    shared_gate = nn(normed_ffn, vmem["w_shared_gate"][...])
    shared_up = nn(normed_ffn, vmem["w_shared_up"][...])
    shared_hidden = (silu(shared_gate) * shared_up).astype(BF16)
    base = hidden + nn(shared_hidden, vmem["w_shared_down"][...])
    latent_new = rms(nn(normed, vmem["w_latent_down"][...]), vmem["g_latent"][...])
    key = nt(normed, vmem["w_rope_key"][...])
    swapped = jnp.concatenate([key[:, half:], key[:, :half]], axis=1)
    key_new = key * cosine[:, :ROPE] + swapped * sine[:, :ROPE]
    kvl = latent_new.shape[1]
    entry_ref[:, 0:kvl] = latent_new.astype(BF16)
    entry_ref[:, kvl : kvl + ROPE] = key_new.astype(BF16)
    route = vmem["route_weights"][...]
    slot_weight = jnp.zeros((slots, rows), F32)
    for k in range(ids.shape[0]):
        hit = slot_expert == ids[k : k + 1, :]
        slot_weight = jnp.where(hit, route[k : k + 1, :], slot_weight)
    slot_weight = jnp.where(spread_ref[...].astype(F32) > 0.5, slot_weight, 0.0)
    high = slot_weight.astype(BF16)
    low = (slot_weight - high.astype(F32)).astype(BF16)
    eye = onehot(iota((rows, rows), 0) == iota((rows, rows), 1))
    weight_high = nt(eye, high).astype(BF16)
    weight_low = nt(eye, low).astype(BF16)
    finish(expert_names)
    for copy in swaps:
        copy.wait()
    gates, ups, downs = (vmem[name] for name in expert_names)

    def serve(low, high):
        steps = range(low * crew, high * crew)
        for e in range(own_experts):
            x = jnp.concatenate(
                [inbox[s, e * CAP : (e + 1) * CAP, :] for s in steps], axis=0
            )
            unit = (silu(nn(x, gates[e])) * nn(x, ups[e])).astype(BF16)
            total = nn(unit, downs[e]).astype(BF16)
            for i, s in enumerate(steps):
                ret_out[s, e * CAP : (e + 1) * CAP, :] = total[i * CAP : (i + 1) * CAP, :]

    def collect(p):
        if crew > 1:
            gate = out_recv.at[2 * p + 1]
            bulk(inbox, p * crew + 1, crew - 1, send_sem.at[0], gate).wait_recv()

        @pl.when(plane != p)
        def _():
            bulk(inbox, p * crew, 1, send_sem.at[0], out_recv.at[2 * p]).wait_recv()

    def give(p):
        @pl.when(plane != p)
        def _():
            back(p, 0).start()

        each(1, crew, lambda i: back(p, i).start())

    chunks = ((0, 1), (1, 2), (2, 3), (3, 4))
    for low, high in chunks if planes == 4 else [(0, planes)]:
        for p in range(low, high):
            collect(p)
        serve(low, high)
        for p in range(low, high):
            give(p)

    ret_in[plane * crew] = ret_out[plane * crew]
    remote = devices - 1
    bulk(ret_in, 0, remote, send_sem.at[1], back_recv.at[0]).wait_recv()
    returned = jnp.concatenate([ret_in[s] for s in range(devices)], axis=0)
    both = nn(weight_high, returned) + nn(weight_low, returned)
    out_ref[...] = (base + both).astype(BF16)
    bulk(outbox, 0, remote, send_sem.at[0], back_recv.at[0]).wait_send()
    bulk(ret_out, 0, remote, send_sem.at[1], back_recv.at[0]).wait_send()


def store_kernel(mixed_ref, entry_ref, out_ref, new_ref, sem):
    copies = (
        pltpu.make_async_copy(mixed_ref, out_ref, sem.at[0]),
        pltpu.make_async_copy(entry_ref, new_ref, sem.at[1]),
    )
    for copy in copies:
        copy.start()
    for copy in copies:
        copy.wait()


NAMES = (
    "tokens", "latent_cache", "rope_cache", "expert_ids", "route_weights", "g_attn",
    "w_query_down", "g_query", "w_latent_down", "g_latent", "w_rope_key", "w_query",
    "w_query_rope", "w_key_up", "w_value_up", "w_out", "g_ffn", "w_expert_gate",
    "w_expert_up", "w_expert_down", "w_shared_gate", "w_shared_up", "w_shared_down",
    "lengths",
)


def local(tokens, latent_cache, rope_cache, lengths, expert_ids, route_weights, *weights):
    named = dict(
        zip(NAMES, (tokens, latent_cache, rope_cache, expert_ids, route_weights) + weights + (lengths,))
    )
    for name in ("g_attn", "g_query", "g_latent", "g_ffn"):
        named[name] = named[name].reshape(1, -1)
    named["rope_cache"] = jnp.swapaxes(rope_cache, 1, 2)
    for name in ("expert_ids", "route_weights", "w_rope_key"):
        named[name] = named[name].T
    ep_size = lax.axis_size("ep")
    tp_size = lax.axis_size("tp")
    devices = ep_size * tp_size
    own = named["w_expert_gate"].shape[0] // tp_size
    rows, width = tokens.shape
    pairs = rows * HEADS
    length, kvl = latent_cache.shape[1:]
    slots = devices * own * CAP

    def holder(name):
        shape = named[name].shape
        if name.startswith("w_expert"):
            axis = 1 if name == "w_expert_down" else 2
            shape = (own,) + tuple(
                n * tp_size if i == axis else n for i, n in enumerate(shape) if i
            )
        if name == "lengths":
            return pltpu.SMEM(shape, named[name].dtype)
        return pltpu.VMEM(shape, named[name].dtype)

    box = pltpu.VMEM((devices, own * CAP, width), BF16)
    dma = pltpu.SemaphoreType.DMA
    mixed, entry = pl.pallas_call(
        functools.partial(step_kernel, ep_size, tp_size, NAMES),
        out_shape=(
            pltpu.VMEM((rows, width), BF16),
            pltpu.VMEM((rows, kvl + ROPE), BF16),
        ),
        in_specs=[pl.BlockSpec(memory_space=pl.ANY)] * len(NAMES),
        out_specs=(pl.BlockSpec(memory_space=pltpu.VMEM),) * 2,
        scratch_shapes=[holder(name) for name in NAMES]
        + [
            pltpu.VMEM((kvl // 128, pairs, 128), F32),
            pltpu.VMEM((pairs, 128), F32),
            pltpu.VMEM((kvl // 128, pairs, 128), F32),
            pltpu.VMEM((rows, kvl, length), BF16),
            pltpu.VMEM((slots, rows), BF16),
            box,
            box,
            box,
            box,
            dma((7,)),
            dma((5,)),
            dma((len(group_sizes(rows)),)),
            dma((3, max(tp_size - 1, 1))),
            dma((3, max(tp_size - 1, 1))),
            dma((2,)),
            dma((2 * (4 if devices % 4 == 0 else 1),)),
            dma((1,)),
        ],
        compiler_params=pltpu.CompilerParams(
            collective_id=0, has_side_effects=True, vmem_limit_bytes=60 * 1024 * 1024
        ),
        name="decode_step",
    )(*[named[name] for name in NAMES])
    return pl.pallas_call(
        store_kernel,
        out_shape=(
            jax.ShapeDtypeStruct(mixed.shape, BF16),
            jax.ShapeDtypeStruct(entry.shape, BF16),
        ),
        in_specs=[pl.BlockSpec(memory_space=pltpu.VMEM)] * 2,
        out_specs=(pl.BlockSpec(memory_space=pl.ANY),) * 2,
        scratch_shapes=[dma((2,))],
        name="store_step",
    )(
        pltpu.with_memory_space_constraint(mixed, pltpu.VMEM),
        pltpu.with_memory_space_constraint(entry, pltpu.VMEM),
    )


def solution(mesh):
    split = ("grp", "ep", "tp")
    in_specs = (
        (P(split, None), P(split, None, None), P(split, None, None), P(split))
        + (P(split, None), P(split, None))
        + (P(),) * 12
        + (P("ep", None, "tp"), P("ep", None, "tp"), P("ep", "tp", None))
        + (P(),) * 3
    )
    out_specs = (P(split, None), P(split, None))
    return jax.shard_map(local, mesh=mesh, in_specs=in_specs, out_specs=out_specs, check_vma=False)
```
